256 devices in a mesh: grp: 4 (over y, x), ep: 32 (over z), tp: 2 (over core).
Axes of the slice: x: 2, y: 2, z: 32, core: 2. Of those that a mesh axis runs over, the one named last changes fastest.
The devices are a block of a 4x16x32 slice.
Arguments:
- tokens: bfloat16 [65536, 2048], P(('grp', 'ep', 'tp')), parts along dimension 0, may hold values from -6 to 6
- norm_gain: float32 [2048], replicated, may hold values from 0.1 to 1.9
- route_ids: int32 [65536, 2], P(('grp', 'ep', 'tp')), parts along dimension 0, may hold values from 0 to 31, as said below
- route_weights: float32 [65536, 2], P(('grp', 'ep', 'tp')), parts along dimension 0, may hold values from 0.1 to 1
- w_gate: bfloat16 [32, 2048, 512], P('ep', None, 'tp'), may hold values from -0.125 to 0.125
- w_up: bfloat16 [32, 2048, 512], P('ep', None, 'tp'), may hold values from -0.125 to 0.125
- w_down: bfloat16 [32, 512, 2048], P('ep', 'tp'), may hold values from -0.25 to 0.25
Outputs:
- mixed: bfloat16 [65536, 2048], P(('grp', 'ep', 'tp')), parts along dimension 0
The draws below stay inside these ranges and needn't reach their ends.
There are 4 independent parts, one for each index of `grp`. The reference program is written for one: setup_inputs(seed, part) draws one part's arguments, and reference() takes and returns one part's arrays. A program takes and returns all parts, laid end to end along the dimension named above; an argument that names none is the same for every part. Nothing has to cross between parts.
Inputs may be any that keep to these rules, and one draw needn't show every extreme that they name: `route_ids`: the 2 experts of a token are different and lie in one group of 8 consecutive experts. Among the tokens of one device (aligned blocks of 256 tokens) no expert is named more than 32 times, and in every such block some expert is named exactly 32 times.
All inputs are finite; a program needn't handle non-finite values.
Results may differ from the reference program's by a relative error of at most 0.007.
Values may be sent and summed in bfloat16 or wider, within the bound.
A program may use at most 128 MiB of HBM per device.

```python
import math
import jax
import jax.numpy as jnp
from jax import lax

D = 2048
FF = 512
GROUPS = 4
TOPK = 2
TOK_DEV = 256
EXPERTS = 32
EXP_GROUP = 8
CAP = 32
TOKENS = 16384


def route_block(block_key):
    subkeys = jax.random.split(block_key, 5)
    halfway = TOK_DEV // 2
    busiest = jax.random.randint(subkeys[0], (), 0, GROUPS)
    spare = halfway - (GROUPS - 1) * EXP_GROUP
    cut_points = jnp.sort(jax.random.randint(subkeys[1], (GROUPS - 2,), 0, spare + 1))
    bounds = jnp.concatenate([jnp.zeros((1,), jnp.int32), cut_points.astype(jnp.int32), jnp.full((1,), spare, jnp.int32)])
    group_sizes = jnp.concatenate([jnp.full((1,), halfway, jnp.int32), bounds[1:] - bounds[:-1] + EXP_GROUP])
    bound_ends = jnp.cumsum(group_sizes)
    starts = bound_ends - group_sizes
    position = jnp.arange(TOK_DEV, dtype=jnp.int32)
    group_rank = jnp.sum((position[:, None] >= bound_ends[None, :]).astype(jnp.int32), axis=1)
    within = position - starts[group_rank]
    group = (busiest + group_rank) % GROUPS
    offsets = jax.random.randint(subkeys[2], (GROUPS,), 0, EXP_GROUP)
    shifts = jax.random.randint(subkeys[3], (GROUPS,), 1, EXP_GROUP)
    first_pick = (within + offsets[group]) % EXP_GROUP
    second_pick = (first_pick + shifts[group]) % EXP_GROUP
    chosen = group[:, None] * EXP_GROUP + jnp.stack([first_pick, second_pick], axis=1)
    shuffle = jax.random.permutation(subkeys[4], TOK_DEV)
    return jnp.zeros((TOK_DEV, 2), jnp.int32).at[shuffle].set(chosen.astype(jnp.int32))


def draw_route_ids(key, part):
    block_keys = jax.random.split(jax.random.fold_in(key, 17), TOKENS // TOK_DEV)
    return jax.vmap(route_block)(block_keys).reshape(TOKENS, TOPK).astype(jnp.int32)


def levels(rng, dims, pieces, smallest, high):
    gain, own = 1.0, jax.random.fold_in(rng, 6)
    for dim, shards_of in pieces:
        steps = jnp.exp(jax.random.uniform(jax.random.fold_in(own, dim), (shards_of,), jnp.float32, smallest / len(pieces), high / len(pieces)))
        gain = gain * jnp.repeat(steps, dims[dim] // shards_of).reshape([-1 if axis == dim else 1 for axis in range(len(dims))])
    return gain


def gaussian(rng, dims, width, reach, pieces=(), held_as=jnp.bfloat16):
    loudness = levels(rng, dims, pieces, -0.22, 0.18) if pieces else 1.0
    result = jax.random.normal(rng, dims, jnp.float32) * width * loudness
    return jnp.minimum(jnp.maximum(result, -reach), reach).astype(held_as)


def setup_inputs(seed: int = 0, part: int = 0) -> dict:
    streams_of = jax.random.split(jax.random.key(seed), 8)
    own_keys = jax.random.split(jax.random.fold_in(streams_of[7], part), 8)
    return {
        "tokens": gaussian(own_keys[0], (TOKENS, D), 1.0, 6.0, ((0, 64),)),
        "norm_gain": jnp.clip(1.0 + 0.18 * jax.random.normal(streams_of[1], (D,), jnp.float32), 0.1, 1.9),
        "route_ids": draw_route_ids(jax.random.fold_in(jax.random.fold_in(streams_of[7], part), 71), part),
        "route_weights": jnp.clip(jnp.exp(math.log(1.0) - 2.3025851 * jax.random.uniform(own_keys[3], (TOKENS, TOPK), jnp.float32) ** levels(own_keys[3], (TOKENS, TOPK), ((0, 64),), -0.2, 0.2)), 0.1, 1.0),
        "w_gate": gaussian(streams_of[4], (EXPERTS, D, FF), D ** -0.5, 0.125, ((0, 32), (2, 2))),
        "w_up": gaussian(streams_of[5], (EXPERTS, D, FF), D ** -0.5, 0.125, ((0, 32), (2, 2))),
        "w_down": gaussian(streams_of[6], (EXPERTS, FF, D), FF ** -0.5, 0.25, ((0, 32), (1, 2))),
    }


epsilon = 1e-06

def reference(tokens, norm_gain, route_ids, route_weights, w_gate, w_up, w_down):
    floats = tokens.astype(jnp.float32)
    inverse = lax.rsqrt(lax.optimization_barrier(jnp.mean(floats * floats, axis=1, keepdims=True)) + epsilon)
    normed = (floats * inverse * norm_gain.astype(jnp.float32)).astype(jnp.bfloat16)
    blocks = TOKENS // TOK_DEV
    route_flat = route_ids.reshape(blocks, TOK_DEV * TOPK).astype(jnp.int32)
    onehot = (route_flat[:, :, None] == jnp.arange(EXPERTS, dtype=jnp.int32)[None, None, :]).astype(jnp.int32)
    slot_index = lax.optimization_barrier(jnp.sum((jnp.cumsum(onehot, axis=1) - onehot) * onehot, axis=2)).astype(jnp.int32)
    anchor = jnp.arange(blocks, dtype=jnp.int32)[:, None]
    position = ((route_flat * blocks + anchor) * CAP + slot_index).astype(jnp.int32)
    position = position.reshape(TOKENS, TOPK)
    buffer = jnp.zeros((EXPERTS * blocks * CAP, D), jnp.bfloat16)
    for column in range(TOPK):
        buffer = buffer.at[position[:, column]].set(normed)
    buffer = buffer.reshape(EXPERTS, blocks * CAP, D)

    def expert(inputs):
        batch_rows, gate_weight, up_weight, down_weight = inputs
        gate_pre = jnp.dot(batch_rows, gate_weight, preferred_element_type=jnp.float32)
        up_pre = jnp.dot(batch_rows, up_weight, preferred_element_type=jnp.float32)
        hidden = (jax.nn.silu(gate_pre) * up_pre).astype(jnp.bfloat16)
        return jnp.dot(hidden, down_weight, preferred_element_type=jnp.float32).astype(jnp.bfloat16)
    results = lax.map(expert, (buffer, w_gate, w_up, w_down)).reshape(EXPERTS * blocks * CAP, D)
    combined = jnp.zeros((TOKENS, D), jnp.float32)
    for column in range(TOPK):
        picked = results[position[:, column]].astype(jnp.float32)
        combined = combined + route_weights[:, column:column + 1].astype(jnp.float32) * picked
    return combined.astype(jnp.bfloat16)
```

```python
import functools

import jax
import jax.numpy as jnp
from jax import lax
from jax.experimental import pallas as pl
from jax.experimental.pallas import tpu as pltpu
from jax.sharding import PartitionSpec as P

GROUPS = 4

epsilon = 1e-06

CHUNK = 16
LAG = 3
CHUNKS = 128
SLOTS = 4
LANES = 128


def send_back(result):
    return lax.all_to_all(result, "ep", split_axis=0, concat_axis=0, tiled=True)


def ring_setup():
    ep = lax.axis_size("ep")
    me = lax.axis_index("ep")
    up, down = lax.rem(me + 1, ep), lax.rem(me + ep - 1, ep)
    barrier = pltpu.get_barrier_semaphore()
    for peer in (up, down):
        pl.semaphore_signal(
            barrier, inc=1, device_id={"ep": peer}, device_id_type=pl.DeviceIdType.MESH
        )
    pl.semaphore_wait(barrier, 2)
    return up, down


def chunk_copy(send, land, send_sem, recv_sem, peer, way, slot, chunk):
    return pltpu.make_async_remote_copy(
        src_ref=send.at[way, slot],
        dst_ref=land.at[way, chunk],
        send_sem=send_sem.at[way, slot],
        recv_sem=recv_sem.at[way, chunk],
        device_id={"ep": peer},
        device_id_type=pl.DeviceIdType.MESH,
    )


def ring_stream(peers, order, build, keep, send, land, send_sem, recv_sem):
    def receive(step):
        for way in (0, 1):
            chunk = order(step)
            chunk_copy(send, land, send_sem, recv_sem, peers[way], way, 0, chunk).wait_recv()
            keep(way, chunk)

    def drain(step):
        slot = lax.rem(step, SLOTS)
        for way in (0, 1):
            chunk_copy(
                send, land, send_sem, recv_sem, peers[way], way, slot, order(step)
            ).wait_send()

    def body(step, carry):
        slot = lax.rem(step, SLOTS)

        @pl.when(step >= LAG)
        def _():
            receive(step - LAG)

        @pl.when(step >= SLOTS)
        def _():
            drain(step - SLOTS)

        for way in (0, 1):
            build(way, slot, order(step))
        for way in (0, 1):
            chunk_copy(
                send, land, send_sem, recv_sem, peers[way], way, slot, order(step)
            ).start()
        return carry

    lax.fori_loop(0, CHUNKS, body, 0)
    for step in range(CHUNKS - LAG, CHUNKS):
        receive(step)
    for step in range(CHUNKS - SLOTS, CHUNKS):
        drain(step)


def dispatch_kernel(
    pick_ref, expert_ref, own_ref, out_ref, store, send, land, send_sem, recv_sem
):
    rows = CHUNKS * CHUNK
    peers = ring_setup()
    own_rows = own_ref.shape[0]

    def take(block, carry):
        at = pl.multiple_of(block * CHUNK, CHUNK)
        store[pl.ds(2 * rows + at, CHUNK)] = own_ref[pl.ds(at, CHUNK)]
        return carry

    lax.fori_loop(0, own_rows // CHUNK, take, 0)
    store[pl.ds(2 * rows + own_rows, 1)] = jnp.zeros((1,) + own_ref.shape[1:], own_ref.dtype)

    def keep(way, chunk):
        store[pl.ds(way * rows + chunk * CHUNK, CHUNK)] = land[way, chunk]

    def build(way, slot, chunk):
        for row in range(CHUNK):
            send[way, slot, row] = store[pick_ref[way, chunk * CHUNK + row]]

    ring_stream(peers, lambda step: step, build, keep, send, land, send_sem, recv_sem)

    def gather(block, carry):
        for row in range(CHUNK):
            at = block * CHUNK + row
            out_ref[at] = store[expert_ref[at]]
        return carry

    lax.fori_loop(0, out_ref.shape[0] // CHUNK, gather, 0)


def collect_kernel(
    result_ref, onward_ref, final_ref, result, out_ref, store, send, land, send_sem, recv_sem
):
    rows = CHUNKS * CHUNK
    up, down = ring_setup()
    store[pl.ds(2 * rows, 1)] = jnp.zeros((1,) + store.shape[1:], store.dtype)

    def keep(way, chunk):
        store[pl.ds(way * rows + chunk * CHUNK, CHUNK)] = land[way, chunk]

    def build(way, slot, chunk):
        for row in range(CHUNK):
            at = chunk * CHUNK + row
            here = result[result_ref[way, at]].astype(jnp.float32)
            beyond = store[onward_ref[way, at]].astype(jnp.float32)
            send[way, slot, row] = (here + beyond).astype(send.dtype)

    ring_stream(
        (down, up),
        lambda step: CHUNKS - 1 - step,
        build,
        keep,
        send,
        land,
        send_sem,
        recv_sem,
    )

    def finish(block, carry):
        for row in range(CHUNK):
            at = block * CHUNK + row
            total = result[final_ref[2, at]].astype(jnp.float32)
            for way in (0, 1):
                total = total + store[final_ref[way, at]].astype(jnp.float32)
            out_ref[at] = total.astype(out_ref.dtype)
        return carry

    lax.fori_loop(0, out_ref.shape[0] // CHUNK, finish, 0)


def ring_call(kernel, name, collective_id, out_rows, store_rows, index_args, data):
    row_shape = data.shape[1:]
    smem = pl.BlockSpec(memory_space=pltpu.SMEM)
    vmem = pl.BlockSpec(memory_space=pltpu.VMEM)
    return pl.pallas_call(
        kernel,
        out_shape=jax.ShapeDtypeStruct((out_rows,) + row_shape, jnp.bfloat16),
        in_specs=[smem] * len(index_args) + [vmem],
        out_specs=vmem,
        scratch_shapes=[
            pltpu.VMEM((store_rows,) + row_shape, jnp.bfloat16),
            pltpu.VMEM((2, SLOTS, CHUNK) + row_shape, jnp.bfloat16),
            pltpu.VMEM((2, CHUNKS, CHUNK) + row_shape, jnp.bfloat16),
            pltpu.SemaphoreType.DMA((2, SLOTS)),
            pltpu.SemaphoreType.DMA((2, CHUNKS)),
        ],
        compiler_params=pltpu.CompilerParams(
            collective_id=collective_id,
            has_side_effects=True,
            vmem_limit_bytes=60 * 1024 * 1024,
        ),
        name=name,
    )(*index_args, data)


def dispatch(pick, expert, own):
    rows = CHUNKS * CHUNK
    return ring_call(
        dispatch_kernel,
        "dispatch",
        0,
        expert.shape[0],
        2 * rows + own.shape[0] + 1,
        (pick, expert),
        own,
    )


def collect(result_pick, onward, final, result):
    rows = CHUNKS * CHUNK
    return ring_call(
        collect_kernel,
        "collect",
        1,
        final.shape[1],
        2 * rows + 1,
        (result_pick, onward, final),
        result,
    )


def plan_routes(route_ids, route_weights, capacity):
    ep = lax.axis_size("ep")
    me = lax.axis_index("ep")
    tokens = route_ids.shape[0]
    steps = ep // 2 + ep // GROUPS
    low = jnp.min(route_ids, axis=1)
    high = jnp.max(route_ids, axis=1)
    ahead = jnp.maximum((low - me) % ep, (high - me) % ep)
    behind = jnp.maximum((me - low) % ep, (me - high) % ep)
    inside = (low <= me) & (me <= high)
    upward = ahead <= behind
    reach = jnp.stack(
        [
            jnp.where(inside, high - me, jnp.where(upward, ahead, 0)),
            jnp.where(inside, me - low, jnp.where(upward, 0, behind)),
        ]
    )
    position = jnp.arange(tokens, dtype=jnp.int32)
    before = position[None, :] < position[:, None]
    further = (reach[:, None, :] > reach[:, :, None]) | (
        (reach[:, None, :] == reach[:, :, None]) & before[None]
    )
    rank = jnp.sum(further.astype(jnp.int32), axis=2)
    alive = jnp.sum(
        (reach[:, :, None] > jnp.arange(steps, dtype=jnp.int32)[None, None, :]).astype(jnp.int32),
        axis=1,
    )
    same = jnp.zeros((tokens, route_ids.shape[1]), jnp.int32)
    for column in range(route_ids.shape[1]):
        match = route_ids[:, :, None] == route_ids[None, None, :, column].reshape(1, 1, tokens)
        same = same + jnp.sum((match & before[:, None, :]).astype(jnp.int32), axis=2)
    target = route_ids * capacity + same
    goes_up = jnp.where(inside[:, None], route_ids > me, upward[:, None])
    code = jnp.where(goes_up, rank[0][:, None], tokens + rank[1][:, None])
    code = jnp.where(route_ids == me, 2 * tokens + position[:, None], code)
    slots = jnp.arange(ep * capacity, dtype=jnp.int32)
    sent_code = jnp.zeros((ep * capacity,), jnp.float32)
    sent_weight = jnp.zeros((ep * capacity,), jnp.float32)
    for column in range(route_ids.shape[1]):
        hit = slots[:, None] == target[None, :, column]
        sent_code = sent_code + jnp.sum(
            jnp.where(hit, (code[:, column] + 1).astype(jnp.float32)[None, :], 0.0), axis=1
        )
        sent_weight = sent_weight + jnp.sum(
            jnp.where(hit, route_weights[:, column][None, :], 0.0), axis=1
        )
    counts = alive.astype(jnp.float32).reshape(1, 2 * steps)
    message = jnp.concatenate(
        [
            sent_code.reshape(ep, capacity),
            sent_weight.reshape(ep, capacity),
            jnp.broadcast_to(counts, (ep, 2 * steps)),
        ],
        axis=1,
    )
    message = jnp.pad(message, ((0, 0), (0, LANES - message.shape[1])))
    return message, reach, rank, target, steps


def lookup(table, index, size):
    choice = index[..., None] == jnp.arange(size, dtype=jnp.int32)
    return jnp.sum(jnp.where(choice, table, 0), axis=-1)


def plan_streams(arrived, reach, rank, target, route_ids, steps, capacity):
    ep = lax.axis_size("ep")
    me = lax.axis_index("ep")
    rows = CHUNKS * CHUNK
    tokens = rank.shape[1]
    codes = arrived[:, :capacity].astype(jnp.int32) - 1
    counts = arrived[:, 2 * capacity : 2 * capacity + 2 * steps].astype(jnp.int32)
    counts = counts.reshape(ep, 2, steps).transpose(1, 2, 0)
    counts = jnp.stack([counts[0], counts[1, :, ::-1]])
    start = jnp.zeros((2, ep), jnp.int32)
    starts, lives = [start], [counts[:, 0]]
    for distance in range(1, steps):
        start = jnp.maximum(
            start + lives[-1], jnp.roll(start, 1, axis=1) + LAG * CHUNK
        )
        starts.append(start)
        lives.append(jnp.roll(counts[:, distance], distance, axis=1))
    starts = jnp.stack(starts, axis=1)
    lives = jnp.stack(lives, axis=1)
    fits = jnp.max(jnp.where(lives > 0, starts + lives, 0)) <= rows

    spot = jnp.stack([me, ep - 1 - me])
    column = jnp.arange(ep, dtype=jnp.int32)

    def at_device(table, device):
        return jnp.sum(jnp.where(column[None, None, :] == device[:, None, None], table, 0), axis=2)

    previous = (spot + ep - 1) % ep
    out_start, out_live = at_device(starts, spot), at_device(lives, spot)
    in_start, in_live = at_device(starts, previous), at_device(lives, previous)
    way_base = (jnp.arange(2, dtype=jnp.int32) * rows)[:, None]
    place = jnp.arange(rows, dtype=jnp.int32)

    def locate(start, live):
        distance = (
            jnp.sum((place[None, :, None] >= start[:, None, :]).astype(jnp.int32), axis=2) - 1
        )
        choice = distance[:, :, None] == jnp.arange(steps, dtype=jnp.int32)
        within = place[None] - jnp.sum(jnp.where(choice, start[:, None, :], 0), axis=2)
        valid = within < jnp.sum(jnp.where(choice, live[:, None, :], 0), axis=2)
        return choice, within, valid

    own_list = jnp.sum(
        jnp.where(
            rank[:, None, :] == jnp.arange(tokens, dtype=jnp.int32)[None, :, None],
            jnp.arange(tokens, dtype=jnp.int32)[None, None, :],
            0,
        ),
        axis=2,
    )
    own_list = jnp.pad(own_list, ((0, 0), (0, rows - tokens)))
    zero_row = 2 * rows + tokens
    choice, within, valid = locate(out_start, out_live)
    shifted = jnp.concatenate([jnp.zeros((2, 1), jnp.int32), in_start[:, :-1]], axis=1)
    source = way_base + within + jnp.sum(jnp.where(choice, shifted[:, None, :], 0), axis=2)
    source = jnp.where(choice[:, :, 0], 2 * rows + own_list, source)
    pick = jnp.clip(jnp.where(valid, source, zero_row), 0, zero_row)

    none_row = 2 * rows
    choice, within, valid = locate(in_start, in_live)
    next_start = jnp.concatenate([out_start[:, 1:], jnp.zeros((2, 1), jnp.int32)], axis=1)
    next_live = jnp.concatenate([out_live[:, 1:], jnp.zeros((2, 1), jnp.int32)], axis=1)
    goes_on = valid & (within < jnp.sum(jnp.where(choice, next_live[:, None, :], 0), axis=2))
    onward = way_base + within + jnp.sum(jnp.where(choice, next_start[:, None, :], 0), axis=2)
    onward = jnp.clip(jnp.where(goes_on, onward, none_row), 0, none_row)

    source_of = jnp.arange(ep, dtype=jnp.int32)
    far = jnp.stack([(me - 1 - source_of) % ep, (source_of - me - 1) % ep])
    base = jnp.stack([lookup(in_start[way], far[way], steps) for way in (0, 1)])
    way_of = (codes >= tokens).astype(jnp.int32)
    spot_of = jnp.where(
        way_of == 1, rows + base[1][:, None] + codes - tokens, base[0][:, None] + codes
    )
    spot_of = jnp.where(codes >= 2 * tokens, 2 * rows + codes - 2 * tokens, spot_of)
    expert = jnp.clip(jnp.where(codes >= 0, spot_of, zero_row), 0, zero_row).reshape(-1)

    total = ep * capacity
    index = jnp.arange(total, dtype=jnp.int32)
    result_pick = jnp.sum(
        jnp.where(
            (way_base + place[None])[:, :, None] == expert[None, None, :],
            index[None, None, :] - total,
            0,
        ),
        axis=2,
    ) + total

    back = jnp.where(reach > 0, way_base + rank, none_row)
    mine = route_ids == me
    local = jnp.sum(jnp.where(mine, target - total, 0), axis=1) + total
    final = jnp.concatenate([jnp.clip(back, 0, none_row), local[None]], axis=0)
    return fits, pick, expert, result_pick, onward, final


def feed_forward(rows, full_gate, full_up, full_down):
    gate_pre = jnp.dot(rows, full_gate, preferred_element_type=jnp.float32)
    up_pre = jnp.dot(rows, full_up, preferred_element_type=jnp.float32)
    hidden = (jax.nn.silu(gate_pre) * up_pre).astype(jnp.bfloat16)
    return jnp.dot(hidden, full_down, preferred_element_type=jnp.float32).astype(jnp.bfloat16)


def padded_exchange(normed, target, route_weights, weights, ep_size, capacity):
    row_count, features = normed.shape
    outbound = jnp.zeros((ep_size * capacity, features), jnp.bfloat16)
    for column in range(target.shape[1]):
        outbound = outbound.at[target[:, column]].set(normed)
    outbound = outbound.reshape(ep_size, capacity, features)
    arrived = lax.all_to_all(outbound, "ep", split_axis=0, concat_axis=0, tiled=True)
    result = feed_forward(arrived.reshape(-1, features), *weights)
    returned_rows = send_back(result.reshape(ep_size, capacity, features))
    returned_rows = returned_rows.reshape(ep_size * capacity, features)
    combined = jnp.zeros((row_count, features), jnp.float32)
    for column in range(target.shape[1]):
        picked = returned_rows[target[:, column]].astype(jnp.float32)
        combined = combined + route_weights[:, column : column + 1] * picked
    return combined.astype(jnp.bfloat16)


def per_device(
    tokens, norm_gain, route_ids, route_weights, w_gate, w_up, w_down, dispatch=dispatch, collect=collect
):
    row_count, features = tokens.shape
    ep_size = lax.axis_size("ep")
    capacity = row_count * GROUPS // ep_size
    floats = tokens.astype(jnp.float32)
    inverse = lax.rsqrt(jnp.mean(floats * floats, axis=1, keepdims=True) + epsilon)
    normed = (floats * inverse * norm_gain).astype(jnp.bfloat16)
    weights = (
        lax.all_gather(w_gate, "tp", axis=2, tiled=True)[0],
        lax.all_gather(w_up, "tp", axis=2, tiled=True)[0],
        lax.all_gather(w_down, "tp", axis=1, tiled=True)[0],
    )
    message, reach, rank, target, steps = plan_routes(route_ids, route_weights, capacity)
    arrived = lax.all_to_all(message, "ep", split_axis=0, concat_axis=0, tiled=True)
    fits, pick, expert, result_pick, onward, final = plan_streams(
        arrived, reach, rank, target, route_ids, steps, capacity
    )
    expert_rows = dispatch(pick, expert, normed.reshape(row_count, -1, LANES))
    result = feed_forward(expert_rows.reshape(-1, features), *weights)
    scale = arrived[:, capacity : 2 * capacity].reshape(-1, 1)
    result = (result.astype(jnp.float32) * scale).astype(jnp.bfloat16)
    result = jnp.pad(result.reshape(-1, features // LANES, LANES), ((0, 1), (0, 0), (0, 0)))
    mixed = collect(result_pick, onward, final, result).reshape(row_count, features)
    return lax.cond(
        fits,
        lambda: mixed,
        lambda: padded_exchange(normed, target, route_weights, weights, ep_size, capacity),
    )


def solution(mesh):
    in_specs = (
        P(("grp", "ep", "tp"), None),
        P(),
        P(("grp", "ep", "tp"), None),
        P(("grp", "ep", "tp"), None),
        P("ep", None, "tp"),
        P("ep", None, "tp"),
        P("ep", "tp", None),
    )
    out_specs = P(("grp", "ep", "tp"), None)
    return jax.shard_map(
        per_device, mesh=mesh, in_specs=in_specs, out_specs=out_specs, check_vma=False
    )
```

```python
import functools

import jax
import jax.numpy as jnp
from jax import lax
from jax.experimental import pallas as pl
from jax.experimental.pallas import tpu as pltpu
from jax.sharding import PartitionSpec as P

GROUPS = 4

epsilon = 1e-06

CHUNK = 16
LAG = 3
CHUNKS = 118
BIAS = 4
SLOTS = 4
LANES = 128


def send_back(result):
    return lax.all_to_all(result, "ep", split_axis=0, concat_axis=0, tiled=True)


def ring_setup(others=()):
    ep = lax.axis_size("ep")
    me = lax.axis_index("ep")
    up, down = lax.rem(me + 1, ep), lax.rem(me + ep - 1, ep)
    peers = [{"ep": up}, {"ep": down}] + list(others)
    barrier = pltpu.get_barrier_semaphore()
    for peer in peers:
        pl.semaphore_signal(
            barrier, inc=1, device_id=peer, device_id_type=pl.DeviceIdType.MESH
        )
    pl.semaphore_wait(barrier, len(peers))
    return up, down


def chunk_copy(send, land, send_sem, recv_sem, peer, way, slot, chunk):
    return pltpu.make_async_remote_copy(
        src_ref=send.at[way, slot],
        dst_ref=land.at[way, chunk],
        send_sem=send_sem.at[way, slot],
        recv_sem=recv_sem.at[way, chunk],
        device_id={"ep": peer},
        device_id_type=pl.DeviceIdType.MESH,
    )


def ring_stream(peers, order, build, keep, send, land, send_sem, recv_sem):
    def receive(step):
        for way in (0, 1):
            chunk = order(step)
            chunk_copy(send, land, send_sem, recv_sem, peers[way], way, 0, chunk).wait_recv()
            keep(way, chunk)

    def drain(step):
        slot = lax.rem(step, SLOTS)
        for way in (0, 1):
            chunk_copy(
                send, land, send_sem, recv_sem, peers[way], way, slot, order(step)
            ).wait_send()

    def body(step, carry):
        slot = lax.rem(step, SLOTS)

        @pl.when(step >= LAG)
        def _():
            receive(step - LAG)

        @pl.when(step >= SLOTS)
        def _():
            drain(step - SLOTS)

        for way in (0, 1):
            build(way, slot, order(step))
        for way in (0, 1):
            chunk_copy(
                send, land, send_sem, recv_sem, peers[way], way, slot, order(step)
            ).start()
        return carry

    lax.fori_loop(0, CHUNKS, body, 0)
    for step in range(CHUNKS - LAG, CHUNKS):
        receive(step)
    for step in range(CHUNKS - SLOTS, CHUNKS):
        drain(step)


def half_copies(halves, wholes, half_sem, own_sem, half, other):
    remote, local = [], []
    for index, (part, whole) in enumerate(zip(halves, wholes)):
        if part.shape[0] == whole.shape[0]:
            width = part.shape[1]
            place = whole.at[:, pl.ds(pl.multiple_of(half * width, width), width)]
        else:
            depth = part.shape[0]
            place = whole.at[pl.ds(pl.multiple_of(half * depth, depth), depth)]
        remote.append(
            pltpu.make_async_remote_copy(
                src_ref=part,
                dst_ref=place,
                send_sem=half_sem.at[0, index],
                recv_sem=half_sem.at[1, index],
                device_id=other,
                device_id_type=pl.DeviceIdType.MESH,
            )
        )
        local.append(pltpu.make_async_copy(part, place, own_sem.at[index]))
    return remote, local


def dispatch_kernel(
    pick_ref,
    expert_ref,
    own_ref,
    gate_half,
    up_half,
    down_half,
    out_ref,
    gate_whole,
    up_whole,
    down_whole,
    store,
    send,
    land,
    send_sem,
    recv_sem,
    half_sem,
    own_sem,
):
    rows = CHUNKS * CHUNK
    half = lax.axis_index("tp")
    other = {"tp": 1 - half}
    peers = ring_setup([other])
    halves = (gate_half, up_half, down_half)
    wholes = (gate_whole, up_whole, down_whole)
    remote, local = half_copies(halves, wholes, half_sem, own_sem, half, other)
    for copy in remote + local:
        copy.start()
    own_rows = own_ref.shape[0]

    def take(block, carry):
        at = pl.multiple_of(block * CHUNK, CHUNK)
        store[pl.ds(2 * rows + at, CHUNK)] = own_ref[pl.ds(at, CHUNK)]
        return carry

    lax.fori_loop(0, own_rows // CHUNK, take, 0)
    store[pl.ds(2 * rows + own_rows, 1)] = jnp.zeros((1,) + own_ref.shape[1:], own_ref.dtype)

    def keep(way, chunk):
        store[pl.ds(way * rows + chunk * CHUNK, CHUNK)] = land[way, chunk]

    def build(way, slot, chunk):
        for row in range(CHUNK):
            send[way, slot, row] = store[pick_ref[way, chunk * CHUNK + row]]

    ring_stream(peers, lambda step: step, build, keep, send, land, send_sem, recv_sem)

    def gather(block, carry):
        for row in range(CHUNK):
            at = block * CHUNK + row
            out_ref[at] = store[expert_ref[at]]
        return carry

    lax.fori_loop(0, out_ref.shape[0] // CHUNK, gather, 0)
    for copy in remote + local:
        copy.wait()


def collect_kernel(
    result_ref, onward_ref, final_ref, result, out_ref, store, send, land, send_sem, recv_sem
):
    rows = CHUNKS * CHUNK
    up, down = ring_setup()
    store[pl.ds(2 * rows, 1)] = jnp.zeros((1,) + store.shape[1:], store.dtype)

    def keep(way, chunk):
        store[pl.ds(way * rows + chunk * CHUNK, CHUNK)] = land[way, chunk]

    def build(way, slot, chunk):
        for row in range(CHUNK):
            at = chunk * CHUNK + row
            here = result[result_ref[way, at]].astype(jnp.float32)
            beyond = store[onward_ref[way, at]].astype(jnp.float32)
            send[way, slot, row] = (here + beyond).astype(send.dtype)

    ring_stream(
        (down, up),
        lambda step: CHUNKS - 1 - step,
        build,
        keep,
        send,
        land,
        send_sem,
        recv_sem,
    )

    def finish(block, carry):
        for row in range(CHUNK):
            at = block * CHUNK + row
            total = result[final_ref[2, at]].astype(jnp.float32)
            for way in (0, 1):
                total = total + store[final_ref[way, at]].astype(jnp.float32)
            out_ref[at] = total.astype(out_ref.dtype)
        return carry

    lax.fori_loop(0, out_ref.shape[0] // CHUNK, finish, 0)


def ring_scratch(store_rows, row_shape):
    return [
        pltpu.VMEM((store_rows,) + row_shape, jnp.bfloat16),
        pltpu.VMEM((2, SLOTS, CHUNK) + row_shape, jnp.bfloat16),
        pltpu.VMEM((2, CHUNKS, CHUNK) + row_shape, jnp.bfloat16),
        pltpu.SemaphoreType.DMA((2, SLOTS)),
        pltpu.SemaphoreType.DMA((2, CHUNKS)),
    ]


def ring_params(collective_id):
    return pltpu.CompilerParams(
        collective_id=collective_id, has_side_effects=True, vmem_limit_bytes=60 * 1024 * 1024
    )


SMEM = pl.BlockSpec(memory_space=pltpu.SMEM)
VMEM = pl.BlockSpec(memory_space=pltpu.VMEM)
ANY = pl.BlockSpec(memory_space=pl.ANY)


def dispatch(pick, expert, own, halves):
    row_shape = own.shape[1:]
    gate_half, up_half, down_half = halves
    wholes = [
        jax.ShapeDtypeStruct((part.shape[0], part.shape[1] * 2), part.dtype)
        for part in (gate_half, up_half)
    ] + [jax.ShapeDtypeStruct((down_half.shape[0] * 2, down_half.shape[1]), down_half.dtype)]
    return pl.pallas_call(
        dispatch_kernel,
        out_shape=[jax.ShapeDtypeStruct((expert.shape[0],) + row_shape, jnp.bfloat16)] + wholes,
        in_specs=[SMEM, SMEM, VMEM, ANY, ANY, ANY],
        out_specs=[VMEM, ANY, ANY, ANY],
        scratch_shapes=ring_scratch(2 * CHUNKS * CHUNK + own.shape[0] + 1, row_shape)
        + [pltpu.SemaphoreType.DMA((2, 3)), pltpu.SemaphoreType.DMA((3,))],
        compiler_params=ring_params(0),
        name="dispatch",
    )(pick, expert, own, *halves)


def collect(result_pick, onward, final, result):
    row_shape = result.shape[1:]
    return pl.pallas_call(
        collect_kernel,
        out_shape=jax.ShapeDtypeStruct((final.shape[1],) + row_shape, jnp.bfloat16),
        in_specs=[SMEM, SMEM, SMEM, VMEM],
        out_specs=VMEM,
        scratch_shapes=ring_scratch(2 * CHUNKS * CHUNK + 1, row_shape),
        compiler_params=ring_params(1),
        name="collect",
    )(result_pick, onward, final, result)


def starts_kernel(steps, counts_ref, starts_ref, lives_ref):
    for way, shift in ((0, 1), (1, LANES - 1)):
        start = jnp.zeros((1, LANES), jnp.int32)
        live = counts_ref[way * steps : way * steps + 1]
        for distance in range(steps):
            if distance:
                start = jnp.maximum(
                    start + live, pltpu.roll(start, shift, axis=1) + LAG * CHUNK
                )
                at = way * steps + distance
                live = pltpu.roll(counts_ref[at : at + 1], shift * distance % LANES, axis=1)
            starts_ref[way * steps + distance : way * steps + distance + 1] = start
            lives_ref[way * steps + distance : way * steps + distance + 1] = live


def stream_starts(counts, steps):
    shape = jax.ShapeDtypeStruct(counts.shape, jnp.int32)
    return pl.pallas_call(
        functools.partial(starts_kernel, steps),
        out_shape=[shape, shape],
        in_specs=[VMEM],
        out_specs=[VMEM, VMEM],
        name="starts",
    )(counts)


def plan_routes(route_ids, route_weights, capacity):
    ep = lax.axis_size("ep")
    me = lax.axis_index("ep")
    tokens = route_ids.shape[0]
    steps = ep // 2 + ep // GROUPS
    low = jnp.min(route_ids, axis=1)
    high = jnp.max(route_ids, axis=1)
    ahead = jnp.maximum((low - me) % ep, (high - me) % ep)
    behind = jnp.maximum((me - low) % ep, (me - high) % ep)
    inside = (low <= me) & (me <= high)
    upward = ahead <= behind
    bias = jnp.arange(-BIAS, BIAS + 1, dtype=jnp.int32)[:, None]
    try_up = (ahead - behind)[None, :] <= bias
    ways = [
        jnp.where(inside, high - me, jnp.where(try_up, ahead, 0)),
        jnp.where(inside, me - low, jnp.where(try_up, 0, behind)),
    ]
    cost = jnp.maximum(jnp.sum(ways[0], axis=1), jnp.sum(ways[1], axis=1))[:, None]
    cost = (cost * 16 + jnp.abs(bias)) * 2 + (bias > 0).astype(jnp.int32)
    best = jnp.sum(jnp.where(cost == jnp.min(cost), bias, 0))
    upward = (ahead - behind) <= best
    reach = jnp.stack(
        [
            jnp.where(inside, high - me, jnp.where(upward, ahead, 0)),
            jnp.where(inside, me - low, jnp.where(upward, 0, behind)),
        ]
    )
    position = jnp.arange(tokens, dtype=jnp.int32)
    before = position[None, :] < position[:, None]
    further = (reach[:, None, :] > reach[:, :, None]) | (
        (reach[:, None, :] == reach[:, :, None]) & before[None]
    )
    rank = jnp.sum(further.astype(jnp.int32), axis=2)
    alive = jnp.sum(
        (reach[:, :, None] > jnp.arange(steps, dtype=jnp.int32)[None, None, :]).astype(jnp.int32),
        axis=1,
    )
    same = jnp.zeros((tokens, route_ids.shape[1]), jnp.int32)
    for column in range(route_ids.shape[1]):
        match = route_ids[:, :, None] == route_ids[None, None, :, column].reshape(1, 1, tokens)
        same = same + jnp.sum((match & before[:, None, :]).astype(jnp.int32), axis=2)
    target = route_ids * capacity + same
    goes_up = jnp.where(inside[:, None], route_ids > me, upward[:, None])
    code = jnp.where(goes_up, rank[0][:, None], tokens + rank[1][:, None])
    code = jnp.where(route_ids == me, 2 * tokens + position[:, None], code)
    slots = jnp.arange(ep * capacity, dtype=jnp.int32)
    sent_code = jnp.zeros((ep * capacity,), jnp.float32)
    sent_weight = jnp.zeros((ep * capacity,), jnp.float32)
    for column in range(route_ids.shape[1]):
        hit = slots[:, None] == target[None, :, column]
        sent_code = sent_code + jnp.sum(
            jnp.where(hit, (code[:, column] + 1).astype(jnp.float32)[None, :], 0.0), axis=1
        )
        sent_weight = sent_weight + jnp.sum(
            jnp.where(hit, route_weights[:, column][None, :], 0.0), axis=1
        )
    counts = alive.astype(jnp.float32).reshape(1, 2 * steps)
    message = jnp.concatenate(
        [
            sent_code.reshape(ep, capacity),
            sent_weight.reshape(ep, capacity),
            jnp.broadcast_to(counts, (ep, 2 * steps)),
        ],
        axis=1,
    )
    message = jnp.pad(message, ((0, 0), (0, LANES - message.shape[1])))
    return message, reach, rank, target, steps


def lookup(table, index, size):
    choice = index[..., None] == jnp.arange(size, dtype=jnp.int32)
    return jnp.sum(jnp.where(choice, table, 0), axis=-1)


def plan_streams(arrived, reach, rank, target, route_ids, steps, capacity, starts_of):
    ep = lax.axis_size("ep")
    me = lax.axis_index("ep")
    rows = CHUNKS * CHUNK
    tokens = rank.shape[1]
    codes = arrived[:, :capacity].astype(jnp.int32) - 1
    counts = arrived[:, 2 * capacity : 2 * capacity + 2 * steps].astype(jnp.int32)
    counts = jnp.tile(counts.T, (1, LANES // ep))
    starts, lives = starts_of(counts, steps)
    starts = starts.reshape(2, steps, LANES)
    lives = lives.reshape(2, steps, LANES)
    fits = jnp.max(jnp.where(lives > 0, starts + lives, 0)) <= rows

    column = jnp.arange(LANES, dtype=jnp.int32)

    def at_device(table, device):
        return jnp.sum(jnp.where(column[None, None, :] == device[:, None, None], table, 0), axis=2)

    spot = jnp.stack([me, me])
    previous = jnp.stack([(me + ep - 1) % ep, (me + 1) % ep])
    out_start, out_live = at_device(starts, spot), at_device(lives, spot)
    in_start, in_live = at_device(starts, previous), at_device(lives, previous)
    way_base = (jnp.arange(2, dtype=jnp.int32) * rows)[:, None]
    place = jnp.arange(rows, dtype=jnp.int32)

    def locate(start, live):
        distance = (
            jnp.sum((place[None, :, None] >= start[:, None, :]).astype(jnp.int32), axis=2) - 1
        )
        choice = distance[:, :, None] == jnp.arange(steps, dtype=jnp.int32)
        within = place[None] - jnp.sum(jnp.where(choice, start[:, None, :], 0), axis=2)
        valid = within < jnp.sum(jnp.where(choice, live[:, None, :], 0), axis=2)
        return choice, within, valid

    own_list = jnp.sum(
        jnp.where(
            rank[:, None, :] == jnp.arange(tokens, dtype=jnp.int32)[None, :, None],
            jnp.arange(tokens, dtype=jnp.int32)[None, None, :],
            0,
        ),
        axis=2,
    )
    own_list = jnp.pad(own_list, ((0, 0), (0, rows - tokens)))
    zero_row = 2 * rows + tokens
    choice, within, valid = locate(out_start, out_live)
    shifted = jnp.concatenate([jnp.zeros((2, 1), jnp.int32), in_start[:, :-1]], axis=1)
    source = way_base + within + jnp.sum(jnp.where(choice, shifted[:, None, :], 0), axis=2)
    source = jnp.where(choice[:, :, 0], 2 * rows + own_list, source)
    pick = jnp.clip(jnp.where(valid, source, zero_row), 0, zero_row)

    none_row = 2 * rows
    choice, within, valid = locate(in_start, in_live)
    next_start = jnp.concatenate([out_start[:, 1:], jnp.zeros((2, 1), jnp.int32)], axis=1)
    next_live = jnp.concatenate([out_live[:, 1:], jnp.zeros((2, 1), jnp.int32)], axis=1)
    goes_on = valid & (within < jnp.sum(jnp.where(choice, next_live[:, None, :], 0), axis=2))
    onward = way_base + within + jnp.sum(jnp.where(choice, next_start[:, None, :], 0), axis=2)
    onward = jnp.clip(jnp.where(goes_on, onward, none_row), 0, none_row)

    source_of = jnp.arange(ep, dtype=jnp.int32)
    far = jnp.stack([(me - 1 - source_of) % ep, (source_of - me - 1) % ep])
    base = jnp.stack([lookup(in_start[way], far[way], steps) for way in (0, 1)])
    way_of = (codes >= tokens).astype(jnp.int32)
    spot_of = jnp.where(
        way_of == 1, rows + base[1][:, None] + codes - tokens, base[0][:, None] + codes
    )
    spot_of = jnp.where(codes >= 2 * tokens, 2 * rows + codes - 2 * tokens, spot_of)
    expert = jnp.clip(jnp.where(codes >= 0, spot_of, zero_row), 0, zero_row).reshape(-1)

    total = ep * capacity
    index = jnp.arange(total, dtype=jnp.int32)
    result_pick = jnp.sum(
        jnp.where(
            (way_base + place[None])[:, :, None] == expert[None, None, :],
            index[None, None, :] - total,
            0,
        ),
        axis=2,
    ) + total

    back = jnp.where(reach > 0, way_base + rank, none_row)
    mine = route_ids == me
    local = jnp.sum(jnp.where(mine, target - total, 0), axis=1) + total
    final = jnp.concatenate([jnp.clip(back, 0, none_row), local[None]], axis=0)
    expert = jnp.pad(expert, (0, CHUNK), constant_values=zero_row)
    return fits, pick, expert, result_pick, onward, final


def feed_forward(rows, full_gate, full_up, full_down):
    gate_pre = jnp.dot(rows, full_gate, preferred_element_type=jnp.float32)
    up_pre = jnp.dot(rows, full_up, preferred_element_type=jnp.float32)
    hidden = (jax.nn.silu(gate_pre) * up_pre).astype(jnp.bfloat16)
    return jnp.dot(hidden, full_down, preferred_element_type=jnp.float32).astype(jnp.bfloat16)


def padded_exchange(normed, target, route_weights, weights, ep_size, capacity):
    row_count, features = normed.shape
    outbound = jnp.zeros((ep_size * capacity, features), jnp.bfloat16)
    for column in range(target.shape[1]):
        outbound = outbound.at[target[:, column]].set(normed)
    outbound = outbound.reshape(ep_size, capacity, features)
    arrived = lax.all_to_all(outbound, "ep", split_axis=0, concat_axis=0, tiled=True)
    result = feed_forward(arrived.reshape(-1, features), *weights)
    returned_rows = send_back(result.reshape(ep_size, capacity, features))
    returned_rows = returned_rows.reshape(ep_size * capacity, features)
    combined = jnp.zeros((row_count, features), jnp.float32)
    for column in range(target.shape[1]):
        picked = returned_rows[target[:, column]].astype(jnp.float32)
        combined = combined + route_weights[:, column : column + 1] * picked
    return combined.astype(jnp.bfloat16)


def per_device(
    tokens,
    norm_gain,
    route_ids,
    route_weights,
    w_gate,
    w_up,
    w_down,
    dispatch=dispatch,
    collect=collect,
    starts_of=stream_starts,
):
    row_count, features = tokens.shape
    ep_size = lax.axis_size("ep")
    capacity = row_count * GROUPS // ep_size
    floats = tokens.astype(jnp.float32)
    inverse = lax.rsqrt(jnp.mean(floats * floats, axis=1, keepdims=True) + epsilon)
    normed = (floats * inverse * norm_gain).astype(jnp.bfloat16)
    message, reach, rank, target, steps = plan_routes(route_ids, route_weights, capacity)
    arrived = lax.all_to_all(message, "ep", split_axis=0, concat_axis=0, tiled=True)
    fits, pick, expert, result_pick, onward, final = plan_streams(
        arrived, reach, rank, target, route_ids, steps, capacity, starts_of
    )
    expert_rows, *weights = dispatch(
        pick, expert, normed.reshape(row_count, -1, LANES), (w_gate[0], w_up[0], w_down[0])
    )
    result = feed_forward(expert_rows.reshape(-1, features), *weights)
    scale = arrived[:, capacity : 2 * capacity].reshape(-1, 1)
    scale = jnp.pad(scale, ((0, CHUNK), (0, 0)))
    result = (result.astype(jnp.float32) * scale).astype(jnp.bfloat16)
    result = result.reshape(-1, features // LANES, LANES)
    mixed = collect(result_pick, onward, final, result).reshape(row_count, features)
    return lax.cond(
        fits,
        lambda: mixed,
        lambda: padded_exchange(normed, target, route_weights, weights, ep_size, capacity),
    )


def solution(mesh):
    in_specs = (
        P(("grp", "ep", "tp"), None),
        P(),
        P(("grp", "ep", "tp"), None),
        P(("grp", "ep", "tp"), None),
        P("ep", None, "tp"),
        P("ep", None, "tp"),
        P("ep", "tp", None),
    )
    out_specs = P(("grp", "ep", "tp"), None)
    return jax.shard_map(
        per_device, mesh=mesh, in_specs=in_specs, out_specs=out_specs, check_vma=False
    )
```

```python
import functools

import jax
import jax.numpy as jnp
from jax import lax
from jax.experimental import pallas as pl
from jax.experimental.pallas import tpu as pltpu
from jax.sharding import PartitionSpec as P

GROUPS = 4

epsilon = 1e-06

CHUNK = 8
LAG = 5
CHUNKS = 232
BIAS = 6
SLOTS = 8
LANES = 128


def send_back(result):
    return lax.all_to_all(result, "ep", split_axis=0, concat_axis=0, tiled=True)


def ring_setup(others=()):
    ep = lax.axis_size("ep")
    me = lax.axis_index("ep")
    up, down = lax.rem(me + 1, ep), lax.rem(me + ep - 1, ep)
    peers = [{"ep": up}, {"ep": down}] + list(others)
    barrier = pltpu.get_barrier_semaphore()
    for peer in peers:
        pl.semaphore_signal(
            barrier, inc=1, device_id=peer, device_id_type=pl.DeviceIdType.MESH
        )
    pl.semaphore_wait(barrier, len(peers))
    return up, down


def chunk_copy(send, land, send_sem, recv_sem, peer, way, slot, chunk):
    return pltpu.make_async_remote_copy(
        src_ref=send.at[way, slot],
        dst_ref=land.at[way, chunk],
        send_sem=send_sem.at[way, slot],
        recv_sem=recv_sem.at[way, chunk],
        device_id={"ep": peer},
        device_id_type=pl.DeviceIdType.MESH,
    )


def ring_stream(peers, order, build, keep, send, land, send_sem, recv_sem):
    def receive(step):
        for way in (0, 1):
            chunk = order(step)
            chunk_copy(send, land, send_sem, recv_sem, peers[way], way, 0, chunk).wait_recv()
            keep(way, chunk)

    def drain(step):
        slot = lax.rem(step, SLOTS)
        for way in (0, 1):
            chunk_copy(
                send, land, send_sem, recv_sem, peers[way], way, slot, order(step)
            ).wait_send()

    def body(step, carry):
        slot = lax.rem(step, SLOTS)

        @pl.when(step >= LAG)
        def _():
            receive(step - LAG)

        @pl.when(step >= SLOTS)
        def _():
            drain(step - SLOTS)

        for way in (0, 1):
            build(way, slot, order(step))
        for way in (0, 1):
            chunk_copy(
                send, land, send_sem, recv_sem, peers[way], way, slot, order(step)
            ).start()
        return carry

    lax.fori_loop(0, CHUNKS, body, 0)
    for step in range(CHUNKS - LAG, CHUNKS):
        receive(step)
    for step in range(CHUNKS - SLOTS, CHUNKS):
        drain(step)


def half_copies(halves, wholes, half_sem, own_sem, half, other):
    remote, local = [], []
    for index, (part, whole) in enumerate(zip(halves, wholes)):
        if part.shape[0] == whole.shape[0]:
            width = part.shape[1]
            place = whole.at[:, pl.ds(pl.multiple_of(half * width, width), width)]
        else:
            depth = part.shape[0]
            place = whole.at[pl.ds(pl.multiple_of(half * depth, depth), depth)]
        remote.append(
            pltpu.make_async_remote_copy(
                src_ref=part,
                dst_ref=place,
                send_sem=half_sem.at[0, index],
                recv_sem=half_sem.at[1, index],
                device_id=other,
                device_id_type=pl.DeviceIdType.MESH,
            )
        )
        local.append(pltpu.make_async_copy(part, place, own_sem.at[index]))
    return remote, local


def dispatch_kernel(
    pick_ref,
    expert_ref,
    own_ref,
    gate_half,
    up_half,
    down_half,
    out_ref,
    gate_whole,
    up_whole,
    down_whole,
    store,
    send,
    land,
    send_sem,
    recv_sem,
    half_sem,
    own_sem,
):
    rows = CHUNKS * CHUNK
    half = lax.axis_index("tp")
    other = {"tp": 1 - half}
    peers = ring_setup([other])
    halves = (gate_half, up_half, down_half)
    wholes = (gate_whole, up_whole, down_whole)
    remote, local = half_copies(halves, wholes, half_sem, own_sem, half, other)
    for copy in remote + local:
        copy.start()
    own_rows = own_ref.shape[0]

    def take(block, carry):
        at = pl.multiple_of(block * CHUNK, CHUNK)
        store[pl.ds(2 * rows + at, CHUNK)] = own_ref[pl.ds(at, CHUNK)]
        return carry

    lax.fori_loop(0, own_rows // CHUNK, take, 0)
    store[pl.ds(2 * rows + own_rows, 1)] = jnp.zeros((1,) + own_ref.shape[1:], own_ref.dtype)

    def keep(way, chunk):
        store[pl.ds(way * rows + chunk * CHUNK, CHUNK)] = land[way, chunk]

    def build(way, slot, chunk):
        for row in range(CHUNK):
            send[way, slot, row] = store[pick_ref[way, chunk * CHUNK + row]]

    ring_stream(peers, lambda step: step, build, keep, send, land, send_sem, recv_sem)

    def gather(block, carry):
        for row in range(CHUNK):
            at = block * CHUNK + row
            out_ref[at] = store[expert_ref[at]]
        return carry

    lax.fori_loop(0, out_ref.shape[0] // CHUNK, gather, 0)
    for copy in remote + local:
        copy.wait()


def collect_kernel(
    result_ref,
    onward_ref,
    final_ref,
    result,
    out_ref,
    store,
    send,
    land,
    send_sem,
    recv_sem,
    load_sem,
):
    rows = CHUNKS * CHUNK
    load = pltpu.make_async_copy(
        result, store.at[pl.ds(2 * rows + CHUNK, result.shape[0])], load_sem
    )
    load.start()
    up, down = ring_setup()
    store[pl.ds(2 * rows, 1)] = jnp.zeros((1,) + store.shape[1:], store.dtype)
    load.wait()

    def keep(way, chunk):
        store[pl.ds(way * rows + chunk * CHUNK, CHUNK)] = land[way, chunk]

    def build(way, slot, chunk):
        for row in range(CHUNK):
            at = chunk * CHUNK + row
            here = store[result_ref[way, at]].astype(jnp.float32)
            beyond = store[onward_ref[way, at]].astype(jnp.float32)
            send[way, slot, row] = (here + beyond).astype(send.dtype)

    ring_stream(
        (down, up),
        lambda step: CHUNKS - 1 - step,
        build,
        keep,
        send,
        land,
        send_sem,
        recv_sem,
    )

    def finish(block, carry):
        for row in range(CHUNK):
            at = block * CHUNK + row
            total = store[final_ref[2, at]].astype(jnp.float32)
            for way in (0, 1):
                total = total + store[final_ref[way, at]].astype(jnp.float32)
            out_ref[at] = total.astype(out_ref.dtype)
        return carry

    lax.fori_loop(0, out_ref.shape[0] // CHUNK, finish, 0)


def ring_scratch(store_rows, row_shape):
    return [
        pltpu.VMEM((store_rows,) + row_shape, jnp.bfloat16),
        pltpu.VMEM((2, SLOTS, CHUNK) + row_shape, jnp.bfloat16),
        pltpu.VMEM((2, CHUNKS, CHUNK) + row_shape, jnp.bfloat16),
        pltpu.SemaphoreType.DMA((2, SLOTS)),
        pltpu.SemaphoreType.DMA((2, CHUNKS)),
    ]


def ring_params(collective_id):
    return pltpu.CompilerParams(
        collective_id=collective_id, has_side_effects=True, vmem_limit_bytes=60 * 1024 * 1024
    )


SMEM = pl.BlockSpec(memory_space=pltpu.SMEM)
VMEM = pl.BlockSpec(memory_space=pltpu.VMEM)
ANY = pl.BlockSpec(memory_space=pl.ANY)


def dispatch(pick, expert, own, halves):
    row_shape = own.shape[1:]
    gate_half, up_half, down_half = halves
    wholes = [
        jax.ShapeDtypeStruct((part.shape[0], part.shape[1] * 2), part.dtype)
        for part in (gate_half, up_half)
    ] + [jax.ShapeDtypeStruct((down_half.shape[0] * 2, down_half.shape[1]), down_half.dtype)]
    return pl.pallas_call(
        dispatch_kernel,
        out_shape=[jax.ShapeDtypeStruct((expert.shape[0],) + row_shape, jnp.bfloat16)] + wholes,
        in_specs=[SMEM, SMEM, VMEM, ANY, ANY, ANY],
        out_specs=[VMEM, ANY, ANY, ANY],
        scratch_shapes=ring_scratch(2 * CHUNKS * CHUNK + own.shape[0] + 1, row_shape)
        + [pltpu.SemaphoreType.DMA((2, 3)), pltpu.SemaphoreType.DMA((3,))],
        compiler_params=ring_params(0),
        name="dispatch",
    )(pick, expert, own, *halves)


def collect(result_pick, onward, final, result):
    row_shape = result.shape[1:]
    return pl.pallas_call(
        collect_kernel,
        out_shape=jax.ShapeDtypeStruct((final.shape[1],) + row_shape, jnp.bfloat16),
        in_specs=[SMEM, SMEM, SMEM, ANY],
        out_specs=VMEM,
        scratch_shapes=ring_scratch(2 * CHUNKS * CHUNK + CHUNK + result.shape[0], row_shape)
        + [pltpu.SemaphoreType.DMA],
        compiler_params=ring_params(1),
        name="collect",
    )(result_pick, onward, final, result)


def starts_kernel(steps, counts_ref, starts_ref, lives_ref):
    for way, shift in ((0, 1), (1, LANES - 1)):
        start = jnp.zeros((1, LANES), jnp.int32)
        live = counts_ref[way * steps : way * steps + 1]
        for distance in range(steps):
            if distance:
                start = jnp.maximum(
                    start + live, pltpu.roll(start, shift, axis=1) + LAG * CHUNK
                )
                at = way * steps + distance
                live = pltpu.roll(counts_ref[at : at + 1], shift * distance % LANES, axis=1)
            starts_ref[way * steps + distance : way * steps + distance + 1] = start
            lives_ref[way * steps + distance : way * steps + distance + 1] = live


def stream_starts(counts, steps):
    shape = jax.ShapeDtypeStruct(counts.shape, jnp.int32)
    return pl.pallas_call(
        functools.partial(starts_kernel, steps),
        out_shape=[shape, shape],
        in_specs=[VMEM],
        out_specs=[VMEM, VMEM],
        name="starts",
    )(counts)


def plan_routes(route_ids, route_weights, capacity):
    ep = lax.axis_size("ep")
    me = lax.axis_index("ep")
    tokens = route_ids.shape[0]
    steps = ep // 2 + ep // GROUPS
    low = jnp.min(route_ids, axis=1)
    high = jnp.max(route_ids, axis=1)
    ahead = jnp.maximum((low - me) % ep, (high - me) % ep)
    behind = jnp.maximum((me - low) % ep, (me - high) % ep)
    inside = (low <= me) & (me <= high)
    upward = ahead <= behind
    bias = jnp.arange(-BIAS, BIAS + 1, dtype=jnp.int32)[:, None]
    try_up = (ahead - behind)[None, :] <= bias
    ways = [
        jnp.where(inside, high - me, jnp.where(try_up, ahead, 0)),
        jnp.where(inside, me - low, jnp.where(try_up, 0, behind)),
    ]
    cost = jnp.maximum(jnp.sum(ways[0], axis=1), jnp.sum(ways[1], axis=1))[:, None]
    cost = (cost * 16 + jnp.abs(bias)) * 2 + (bias > 0).astype(jnp.int32)
    best = jnp.sum(jnp.where(cost == jnp.min(cost), bias, 0))
    upward = (ahead - behind) <= best
    reach = jnp.stack(
        [
            jnp.where(inside, high - me, jnp.where(upward, ahead, 0)),
            jnp.where(inside, me - low, jnp.where(upward, 0, behind)),
        ]
    )
    position = jnp.arange(tokens, dtype=jnp.int32)
    before = position[None, :] < position[:, None]
    further = (reach[:, None, :] > reach[:, :, None]) | (
        (reach[:, None, :] == reach[:, :, None]) & before[None]
    )
    rank = jnp.sum(further.astype(jnp.int32), axis=2)
    alive = jnp.sum(
        (reach[:, :, None] > jnp.arange(steps, dtype=jnp.int32)[None, None, :]).astype(jnp.int32),
        axis=1,
    )
    same = jnp.zeros((tokens, route_ids.shape[1]), jnp.int32)
    for column in range(route_ids.shape[1]):
        match = route_ids[:, :, None] == route_ids[None, None, :, column].reshape(1, 1, tokens)
        same = same + jnp.sum((match & before[:, None, :]).astype(jnp.int32), axis=2)
    target = route_ids * capacity + same
    goes_up = jnp.where(inside[:, None], route_ids > me, upward[:, None])
    code = jnp.where(goes_up, rank[0][:, None], tokens + rank[1][:, None])
    code = jnp.where(route_ids == me, 2 * tokens + position[:, None], code)
    slots = jnp.arange(ep * capacity, dtype=jnp.int32)
    sent_code = jnp.zeros((ep * capacity,), jnp.float32)
    sent_weight = jnp.zeros((ep * capacity,), jnp.float32)
    for column in range(route_ids.shape[1]):
        hit = slots[:, None] == target[None, :, column]
        sent_code = sent_code + jnp.sum(
            jnp.where(hit, (code[:, column] + 1).astype(jnp.float32)[None, :], 0.0), axis=1
        )
        sent_weight = sent_weight + jnp.sum(
            jnp.where(hit, route_weights[:, column][None, :], 0.0), axis=1
        )
    counts = alive.astype(jnp.float32).reshape(1, 2 * steps)
    message = jnp.concatenate(
        [
            sent_code.reshape(ep, capacity),
            sent_weight.reshape(ep, capacity),
            jnp.broadcast_to(counts, (ep, 2 * steps)),
        ],
        axis=1,
    )
    message = jnp.pad(message, ((0, 0), (0, LANES - message.shape[1])))
    return message, reach, rank, target, steps


def lookup(table, index, size):
    choice = index[..., None] == jnp.arange(size, dtype=jnp.int32)
    return jnp.sum(jnp.where(choice, table, 0), axis=-1)


def plan_streams(arrived, reach, rank, target, route_ids, steps, capacity, starts_of):
    ep = lax.axis_size("ep")
    me = lax.axis_index("ep")
    rows = CHUNKS * CHUNK
    tokens = rank.shape[1]
    codes = arrived[:, :capacity].astype(jnp.int32) - 1
    counts = arrived[:, 2 * capacity : 2 * capacity + 2 * steps].astype(jnp.int32)
    counts = jnp.tile(counts.T, (1, LANES // ep))
    starts, lives = starts_of(counts, steps)
    starts = starts.reshape(2, steps, LANES)
    lives = lives.reshape(2, steps, LANES)
    fits = jnp.max(jnp.where(lives > 0, starts + lives, 0)) <= rows

    column = jnp.arange(LANES, dtype=jnp.int32)

    def at_device(table, device):
        return jnp.sum(jnp.where(column[None, None, :] == device[:, None, None], table, 0), axis=2)

    spot = jnp.stack([me, me])
    previous = jnp.stack([(me + ep - 1) % ep, (me + 1) % ep])
    out_start, out_live = at_device(starts, spot), at_device(lives, spot)
    in_start, in_live = at_device(starts, previous), at_device(lives, previous)
    way_base = (jnp.arange(2, dtype=jnp.int32) * rows)[:, None]
    place = jnp.arange(rows, dtype=jnp.int32)

    def locate(start, live):
        distance = (
            jnp.sum((place[None, :, None] >= start[:, None, :]).astype(jnp.int32), axis=2) - 1
        )
        choice = distance[:, :, None] == jnp.arange(steps, dtype=jnp.int32)
        within = place[None] - jnp.sum(jnp.where(choice, start[:, None, :], 0), axis=2)
        valid = within < jnp.sum(jnp.where(choice, live[:, None, :], 0), axis=2)
        return choice, within, valid

    own_list = jnp.sum(
        jnp.where(
            rank[:, None, :] == jnp.arange(tokens, dtype=jnp.int32)[None, :, None],
            jnp.arange(tokens, dtype=jnp.int32)[None, None, :],
            0,
        ),
        axis=2,
    )
    own_list = jnp.pad(own_list, ((0, 0), (0, rows - tokens)))
    zero_row = 2 * rows + tokens
    choice, within, valid = locate(out_start, out_live)
    shifted = jnp.concatenate([jnp.zeros((2, 1), jnp.int32), in_start[:, :-1]], axis=1)
    source = way_base + within + jnp.sum(jnp.where(choice, shifted[:, None, :], 0), axis=2)
    source = jnp.where(choice[:, :, 0], 2 * rows + own_list, source)
    pick = jnp.clip(jnp.where(valid, source, zero_row), 0, zero_row)

    none_row = 2 * rows
    choice, within, valid = locate(in_start, in_live)
    next_start = jnp.concatenate([out_start[:, 1:], jnp.zeros((2, 1), jnp.int32)], axis=1)
    next_live = jnp.concatenate([out_live[:, 1:], jnp.zeros((2, 1), jnp.int32)], axis=1)
    goes_on = valid & (within < jnp.sum(jnp.where(choice, next_live[:, None, :], 0), axis=2))
    onward = way_base + within + jnp.sum(jnp.where(choice, next_start[:, None, :], 0), axis=2)
    onward = jnp.clip(jnp.where(goes_on, onward, none_row), 0, none_row)

    source_of = jnp.arange(ep, dtype=jnp.int32)
    far = jnp.stack([(me - 1 - source_of) % ep, (source_of - me - 1) % ep])
    base = jnp.stack([lookup(in_start[way], far[way], steps) for way in (0, 1)])
    way_of = (codes >= tokens).astype(jnp.int32)
    spot_of = jnp.where(
        way_of == 1, rows + base[1][:, None] + codes - tokens, base[0][:, None] + codes
    )
    spot_of = jnp.where(codes >= 2 * tokens, 2 * rows + codes - 2 * tokens, spot_of)
    expert = jnp.clip(jnp.where(codes >= 0, spot_of, zero_row), 0, zero_row).reshape(-1)

    total = ep * capacity
    index = jnp.arange(total, dtype=jnp.int32) + 1
    here = (expert[:, None] // CHUNK == jnp.arange(2 * CHUNKS, dtype=jnp.int32)[None]).astype(
        jnp.bfloat16
    )
    inner = expert[:, None] % CHUNK == jnp.arange(CHUNK, dtype=jnp.int32)[None]
    parts = [
        jnp.where(inner, part[:, None], 0).astype(jnp.bfloat16)
        for part in (index // LANES, index % LANES)
    ]
    found = lax.dot_general(
        here,
        jnp.concatenate(parts, axis=1),
        (((0,), (0,)), ((), ())),
        preferred_element_type=jnp.float32,
    ).astype(jnp.int32)
    found = (found[:, :CHUNK] * LANES + found[:, CHUNK:]).reshape(2, rows)
    first_result = none_row + CHUNK
    result_pick = jnp.where(found > 0, first_result + found - 1, none_row)

    back = jnp.where(reach > 0, way_base + rank, none_row)
    mine = route_ids == me
    local = jnp.sum(jnp.where(mine, first_result + target - none_row, 0), axis=1) + none_row
    final = jnp.concatenate([jnp.clip(back, 0, none_row), local[None]], axis=0)
    return fits, pick, expert, result_pick, onward, final


def feed_forward(rows, full_gate, full_up, full_down):
    gate_pre = jnp.dot(rows, full_gate, preferred_element_type=jnp.float32)
    up_pre = jnp.dot(rows, full_up, preferred_element_type=jnp.float32)
    hidden = (jax.nn.silu(gate_pre) * up_pre).astype(jnp.bfloat16)
    return jnp.dot(hidden, full_down, preferred_element_type=jnp.float32).astype(jnp.bfloat16)


def padded_exchange(normed, target, route_weights, weights, ep_size, capacity):
    row_count, features = normed.shape
    outbound = jnp.zeros((ep_size * capacity, features), jnp.bfloat16)
    for column in range(target.shape[1]):
        outbound = outbound.at[target[:, column]].set(normed)
    outbound = outbound.reshape(ep_size, capacity, features)
    arrived = lax.all_to_all(outbound, "ep", split_axis=0, concat_axis=0, tiled=True)
    result = feed_forward(arrived.reshape(-1, features), *weights)
    returned_rows = send_back(result.reshape(ep_size, capacity, features))
    returned_rows = returned_rows.reshape(ep_size * capacity, features)
    combined = jnp.zeros((row_count, features), jnp.float32)
    for column in range(target.shape[1]):
        picked = returned_rows[target[:, column]].astype(jnp.float32)
        combined = combined + route_weights[:, column : column + 1] * picked
    return combined.astype(jnp.bfloat16)


def per_device(
    tokens,
    norm_gain,
    route_ids,
    route_weights,
    w_gate,
    w_up,
    w_down,
    dispatch=dispatch,
    collect=collect,
    starts_of=stream_starts,
):
    row_count, features = tokens.shape
    ep_size = lax.axis_size("ep")
    capacity = row_count * GROUPS // ep_size
    floats = tokens.astype(jnp.float32)
    inverse = lax.rsqrt(jnp.mean(floats * floats, axis=1, keepdims=True) + epsilon)
    normed = (floats * inverse * norm_gain).astype(jnp.bfloat16)
    message, reach, rank, target, steps = plan_routes(route_ids, route_weights, capacity)
    arrived = lax.all_to_all(message, "ep", split_axis=0, concat_axis=0, tiled=True)
    fits, pick, expert, result_pick, onward, final = plan_streams(
        arrived, reach, rank, target, route_ids, steps, capacity, starts_of
    )
    expert_rows, *weights = dispatch(
        pick, expert, normed.reshape(row_count, -1, LANES), (w_gate[0], w_up[0], w_down[0])
    )
    result = feed_forward(expert_rows.reshape(-1, features), *weights)
    scale = arrived[:, capacity : 2 * capacity].reshape(-1, 1)
    result = (result.astype(jnp.float32) * scale).astype(jnp.bfloat16)
    result = result.reshape(-1, features // LANES, LANES)
    mixed = collect(result_pick, onward, final, result).reshape(row_count, features)
    return lax.cond(
        fits,
        lambda: mixed,
        lambda: padded_exchange(normed, target, route_weights, weights, ep_size, capacity),
    )


def solution(mesh):
    in_specs = (
        P(("grp", "ep", "tp"), None),
        P(),
        P(("grp", "ep", "tp"), None),
        P(("grp", "ep", "tp"), None),
        P("ep", None, "tp"),
        P("ep", None, "tp"),
        P("ep", "tp", None),
    )
    out_specs = P(("grp", "ep", "tp"), None)
    return jax.shard_map(
        per_device, mesh=mesh, in_specs=in_specs, out_specs=out_specs, check_vma=False
    )
```

```python
import functools

import jax
import jax.numpy as jnp
from jax import lax
from jax.experimental import pallas as pl
from jax.experimental.pallas import tpu as pltpu
from jax.sharding import PartitionSpec as P

GROUPS = 4

epsilon = 1e-06

CHUNK = 8
LAG = 6
CHUNKS = 238
BIAS = 6
SLOTS = 8
LANES = 128


def send_back(result):
    return lax.all_to_all(result, "ep", split_axis=0, concat_axis=0, tiled=True)


def ring_setup(others=()):
    ep = lax.axis_size("ep")
    me = lax.axis_index("ep")
    up, down = lax.rem(me + 1, ep), lax.rem(me + ep - 1, ep)
    peers = [{"ep": up}, {"ep": down}] + list(others)
    barrier = pltpu.get_barrier_semaphore()
    for peer in peers:
        pl.semaphore_signal(
            barrier, inc=1, device_id=peer, device_id_type=pl.DeviceIdType.MESH
        )
    pl.semaphore_wait(barrier, len(peers))
    return up, down


def chunk_copy(send, land, send_sem, recv_sem, peer, way, slot, chunk):
    return pltpu.make_async_remote_copy(
        src_ref=send.at[way, slot],
        dst_ref=land.at[way, chunk],
        send_sem=send_sem.at[way, slot],
        recv_sem=recv_sem.at[way, chunk],
        device_id={"ep": peer},
        device_id_type=pl.DeviceIdType.MESH,
    )


def ring_stream(peers, order, build, keep, send, land, send_sem, recv_sem):
    def receive(step):
        for way in (0, 1):
            chunk = order(step)
            chunk_copy(send, land, send_sem, recv_sem, peers[way], way, 0, chunk).wait_recv()
            keep(way, chunk)

    def drain(step):
        slot = lax.rem(step, SLOTS)
        for way in (0, 1):
            chunk_copy(
                send, land, send_sem, recv_sem, peers[way], way, slot, order(step)
            ).wait_send()

    def body(step, carry):
        slot = lax.rem(step, SLOTS)

        @pl.when(step >= LAG)
        def _():
            receive(step - LAG)

        @pl.when(step >= SLOTS)
        def _():
            drain(step - SLOTS)

        for way in (0, 1):
            build(way, slot, order(step))
        for way in (0, 1):
            chunk_copy(
                send, land, send_sem, recv_sem, peers[way], way, slot, order(step)
            ).start()
        return carry

    lax.fori_loop(0, CHUNKS, body, 0)
    for step in range(CHUNKS - LAG, CHUNKS):
        receive(step)
    for step in range(CHUNKS - SLOTS, CHUNKS):
        drain(step)


def half_copies(halves, wholes, half_sem, own_sem, half, other):
    remote, local = [], []
    for index, (part, whole, group) in enumerate(zip(halves, wholes, (0, 1, 0))):
        if part.shape[0] == whole.shape[0]:
            width = part.shape[1]
            at = (2 * group + half) * width
            place = whole.at[:, pl.ds(pl.multiple_of(at, width), width)]
        else:
            depth = part.shape[0]
            place = whole.at[pl.ds(pl.multiple_of(half * depth, depth), depth)]
        remote.append(
            pltpu.make_async_remote_copy(
                src_ref=part,
                dst_ref=place,
                send_sem=half_sem.at[0, index],
                recv_sem=half_sem.at[1, index],
                device_id=other,
                device_id_type=pl.DeviceIdType.MESH,
            )
        )
        local.append(pltpu.make_async_copy(part, place, own_sem.at[index]))
    return remote, local


def dispatch_kernel(
    pick_ref,
    expert_ref,
    own_ref,
    gate_half,
    up_half,
    down_half,
    out_ref,
    gate_up_whole,
    down_whole,
    store,
    send,
    land,
    send_sem,
    recv_sem,
    half_sem,
    own_sem,
):
    rows = CHUNKS * CHUNK
    half = lax.axis_index("tp")
    other = {"tp": 1 - half}
    peers = ring_setup([other])
    halves = (gate_half, up_half, down_half)
    wholes = (gate_up_whole, gate_up_whole, down_whole)
    remote, local = half_copies(halves, wholes, half_sem, own_sem, half, other)
    for copy in remote + local:
        copy.start()
    own_rows = own_ref.shape[0]

    def take(block, carry):
        at = pl.multiple_of(block * CHUNK, CHUNK)
        store[pl.ds(2 * rows + at, CHUNK)] = own_ref[pl.ds(at, CHUNK)]
        return carry

    lax.fori_loop(0, own_rows // CHUNK, take, 0)
    store[pl.ds(2 * rows + own_rows, 1)] = jnp.zeros((1,) + own_ref.shape[1:], own_ref.dtype)

    def keep(way, chunk):
        store[pl.ds(way * rows + chunk * CHUNK, CHUNK)] = land[way, chunk]

    def build(way, slot, chunk):
        for row in range(CHUNK):
            send[way, slot, row] = store[pick_ref[way, chunk * CHUNK + row]]

    ring_stream(peers, lambda step: step, build, keep, send, land, send_sem, recv_sem)

    def gather(block, carry):
        for row in range(CHUNK):
            at = block * CHUNK + row
            out_ref[at] = store[expert_ref[at]]
        return carry

    lax.fori_loop(0, out_ref.shape[0] // CHUNK, gather, 0)
    for copy in remote + local:
        copy.wait()


def collect_kernel(
    result_ref,
    onward_ref,
    final_ref,
    result,
    out_ref,
    store,
    send,
    land,
    send_sem,
    recv_sem,
    load_sem,
):
    rows = CHUNKS * CHUNK
    load = pltpu.make_async_copy(
        result, store.at[pl.ds(2 * rows + CHUNK, result.shape[0])], load_sem
    )
    load.start()
    up, down = ring_setup()
    store[pl.ds(2 * rows, 1)] = jnp.zeros((1,) + store.shape[1:], store.dtype)
    load.wait()

    def keep(way, chunk):
        store[pl.ds(way * rows + chunk * CHUNK, CHUNK)] = land[way, chunk]

    def build(way, slot, chunk):
        for row in range(CHUNK):
            at = chunk * CHUNK + row
            here = store[result_ref[way, at]].astype(jnp.float32)
            beyond = store[onward_ref[way, at]].astype(jnp.float32)
            send[way, slot, row] = (here + beyond).astype(send.dtype)

    ring_stream(
        (down, up),
        lambda step: CHUNKS - 1 - step,
        build,
        keep,
        send,
        land,
        send_sem,
        recv_sem,
    )

    def finish(block, carry):
        for row in range(CHUNK):
            at = block * CHUNK + row
            total = store[final_ref[2, at]].astype(jnp.float32)
            for way in (0, 1):
                total = total + store[final_ref[way, at]].astype(jnp.float32)
            out_ref[at] = total.astype(out_ref.dtype)
        return carry

    lax.fori_loop(0, out_ref.shape[0] // CHUNK, finish, 0)


def ring_scratch(store_rows, row_shape):
    return [
        pltpu.VMEM((store_rows,) + row_shape, jnp.bfloat16),
        pltpu.VMEM((2, SLOTS, CHUNK) + row_shape, jnp.bfloat16),
        pltpu.VMEM((2, CHUNKS, CHUNK) + row_shape, jnp.bfloat16),
        pltpu.SemaphoreType.DMA((2, SLOTS)),
        pltpu.SemaphoreType.DMA((2, CHUNKS)),
    ]


def ring_params(collective_id):
    return pltpu.CompilerParams(
        collective_id=collective_id, has_side_effects=True, vmem_limit_bytes=60 * 1024 * 1024
    )


SMEM = pl.BlockSpec(memory_space=pltpu.SMEM)
VMEM = pl.BlockSpec(memory_space=pltpu.VMEM)
ANY = pl.BlockSpec(memory_space=pl.ANY)


def dispatch(pick, expert, own, halves):
    row_shape = own.shape[1:]
    gate_half, _, down_half = halves
    wholes = [
        jax.ShapeDtypeStruct((gate_half.shape[0], 4 * gate_half.shape[1]), gate_half.dtype),
        jax.ShapeDtypeStruct((down_half.shape[0] * 2, down_half.shape[1]), down_half.dtype),
    ]
    return pl.pallas_call(
        dispatch_kernel,
        out_shape=[jax.ShapeDtypeStruct((expert.shape[0],) + row_shape, jnp.bfloat16)] + wholes,
        in_specs=[SMEM, SMEM, VMEM, ANY, ANY, ANY],
        out_specs=[VMEM, ANY, ANY],
        scratch_shapes=ring_scratch(2 * CHUNKS * CHUNK + own.shape[0] + 1, row_shape)
        + [pltpu.SemaphoreType.DMA((2, 3)), pltpu.SemaphoreType.DMA((3,))],
        compiler_params=ring_params(0),
        name="dispatch",
    )(pick, expert, own, *halves)


def collect(result_pick, onward, final, result):
    row_shape = result.shape[1:]
    return pl.pallas_call(
        collect_kernel,
        out_shape=jax.ShapeDtypeStruct((final.shape[1],) + row_shape, jnp.bfloat16),
        in_specs=[SMEM, SMEM, SMEM, ANY],
        out_specs=VMEM,
        scratch_shapes=ring_scratch(2 * CHUNKS * CHUNK + CHUNK + result.shape[0], row_shape)
        + [pltpu.SemaphoreType.DMA],
        compiler_params=ring_params(1),
        name="collect",
    )(result_pick, onward, final, result)


def starts_kernel(steps, counts_ref, starts_ref, lives_ref):
    for way, shift in ((0, 1), (1, LANES - 1)):
        start = jnp.zeros((1, LANES), jnp.int32)
        live = counts_ref[way * steps : way * steps + 1]
        for distance in range(steps):
            if distance:
                start = jnp.maximum(
                    start + live, pltpu.roll(start, shift, axis=1) + LAG * CHUNK
                )
                at = way * steps + distance
                live = pltpu.roll(counts_ref[at : at + 1], shift * distance % LANES, axis=1)
            starts_ref[way * steps + distance : way * steps + distance + 1] = start
            lives_ref[way * steps + distance : way * steps + distance + 1] = live


def stream_starts(counts, steps):
    shape = jax.ShapeDtypeStruct(counts.shape, jnp.int32)
    return pl.pallas_call(
        functools.partial(starts_kernel, steps),
        out_shape=[shape, shape],
        in_specs=[VMEM],
        out_specs=[VMEM, VMEM],
        name="starts",
    )(counts)


def plan_routes(route_ids, route_weights, capacity):
    ep = lax.axis_size("ep")
    me = lax.axis_index("ep")
    tokens = route_ids.shape[0]
    steps = ep // 2 + ep // GROUPS
    low = jnp.min(route_ids, axis=1)
    high = jnp.max(route_ids, axis=1)
    ahead = jnp.maximum((low - me) % ep, (high - me) % ep)
    behind = jnp.maximum((me - low) % ep, (me - high) % ep)
    inside = (low <= me) & (me <= high)
    upward = ahead <= behind
    bias = jnp.arange(-BIAS, BIAS + 1, dtype=jnp.int32)[:, None]
    try_up = (ahead - behind)[None, :] <= bias
    ways = [
        jnp.where(inside, high - me, jnp.where(try_up, ahead, 0)),
        jnp.where(inside, me - low, jnp.where(try_up, 0, behind)),
    ]
    cost = jnp.maximum(jnp.sum(ways[0], axis=1), jnp.sum(ways[1], axis=1))[:, None]
    cost = (cost * 16 + jnp.abs(bias)) * 2 + (bias > 0).astype(jnp.int32)
    best = jnp.sum(jnp.where(cost == jnp.min(cost), bias, 0))
    upward = (ahead - behind) <= best
    reach = jnp.stack(
        [
            jnp.where(inside, high - me, jnp.where(upward, ahead, 0)),
            jnp.where(inside, me - low, jnp.where(upward, 0, behind)),
        ]
    )
    position = jnp.arange(tokens, dtype=jnp.int32)
    before = position[None, :] < position[:, None]
    further = (reach[:, None, :] > reach[:, :, None]) | (
        (reach[:, None, :] == reach[:, :, None]) & before[None]
    )
    rank = jnp.sum(further.astype(jnp.int32), axis=2)
    alive = jnp.sum(
        (reach[:, :, None] > jnp.arange(steps, dtype=jnp.int32)[None, None, :]).astype(jnp.int32),
        axis=1,
    )
    same = jnp.zeros((tokens, route_ids.shape[1]), jnp.int32)
    for column in range(route_ids.shape[1]):
        match = route_ids[:, :, None] == route_ids[None, None, :, column].reshape(1, 1, tokens)
        same = same + jnp.sum((match & before[:, None, :]).astype(jnp.int32), axis=2)
    target = route_ids * capacity + same
    goes_up = jnp.where(inside[:, None], route_ids > me, upward[:, None])
    code = jnp.where(goes_up, rank[0][:, None], tokens + rank[1][:, None])
    code = jnp.where(route_ids == me, 2 * tokens + position[:, None], code)
    slots = jnp.arange(ep * capacity, dtype=jnp.int32)
    sent_code = jnp.zeros((ep * capacity,), jnp.float32)
    sent_weight = jnp.zeros((ep * capacity,), jnp.float32)
    for column in range(route_ids.shape[1]):
        hit = slots[:, None] == target[None, :, column]
        sent_code = sent_code + jnp.sum(
            jnp.where(hit, (code[:, column] + 1).astype(jnp.float32)[None, :], 0.0), axis=1
        )
        sent_weight = sent_weight + jnp.sum(
            jnp.where(hit, route_weights[:, column][None, :], 0.0), axis=1
        )
    counts = alive.astype(jnp.float32).reshape(1, 2 * steps)
    message = jnp.concatenate(
        [
            sent_code.reshape(ep, capacity),
            sent_weight.reshape(ep, capacity),
            jnp.broadcast_to(counts, (ep, 2 * steps)),
        ],
        axis=1,
    )
    message = jnp.pad(message, ((0, 0), (0, LANES - message.shape[1])))
    return message, reach, rank, target, steps


def lookup(table, index, size):
    choice = index[..., None] == jnp.arange(size, dtype=jnp.int32)
    return jnp.sum(jnp.where(choice, table, 0), axis=-1)


def plan_streams(arrived, reach, rank, target, route_ids, steps, capacity, starts_of):
    ep = lax.axis_size("ep")
    me = lax.axis_index("ep")
    rows = CHUNKS * CHUNK
    tokens = rank.shape[1]
    codes = arrived[:, :capacity].astype(jnp.int32) - 1
    counts = arrived[:, 2 * capacity : 2 * capacity + 2 * steps].astype(jnp.int32)
    counts = jnp.tile(counts.T, (1, LANES // ep))
    starts, lives = starts_of(counts, steps)
    starts = starts.reshape(2, steps, LANES)
    lives = lives.reshape(2, steps, LANES)
    fits = jnp.max(jnp.where(lives > 0, starts + lives, 0)) <= rows

    column = jnp.arange(LANES, dtype=jnp.int32)

    def at_device(table, device):
        return jnp.sum(jnp.where(column[None, None, :] == device[:, None, None], table, 0), axis=2)

    spot = jnp.stack([me, me])
    previous = jnp.stack([(me + ep - 1) % ep, (me + 1) % ep])
    out_start, out_live = at_device(starts, spot), at_device(lives, spot)
    in_start, in_live = at_device(starts, previous), at_device(lives, previous)
    way_base = (jnp.arange(2, dtype=jnp.int32) * rows)[:, None]
    place = jnp.arange(rows, dtype=jnp.int32)

    def locate(start, live):
        distance = (
            jnp.sum((place[None, :, None] >= start[:, None, :]).astype(jnp.int32), axis=2) - 1
        )
        choice = distance[:, :, None] == jnp.arange(steps, dtype=jnp.int32)
        within = place[None] - jnp.sum(jnp.where(choice, start[:, None, :], 0), axis=2)
        valid = within < jnp.sum(jnp.where(choice, live[:, None, :], 0), axis=2)
        return choice, within, valid

    own_list = jnp.sum(
        jnp.where(
            rank[:, None, :] == jnp.arange(tokens, dtype=jnp.int32)[None, :, None],
            jnp.arange(tokens, dtype=jnp.int32)[None, None, :],
            0,
        ),
        axis=2,
    )
    own_list = jnp.pad(own_list, ((0, 0), (0, rows - tokens)))
    zero_row = 2 * rows + tokens
    choice, within, valid = locate(out_start, out_live)
    shifted = jnp.concatenate([jnp.zeros((2, 1), jnp.int32), in_start[:, :-1]], axis=1)
    source = way_base + within + jnp.sum(jnp.where(choice, shifted[:, None, :], 0), axis=2)
    source = jnp.where(choice[:, :, 0], 2 * rows + own_list, source)
    pick = jnp.clip(jnp.where(valid, source, zero_row), 0, zero_row)

    none_row = 2 * rows
    choice, within, valid = locate(in_start, in_live)
    next_start = jnp.concatenate([out_start[:, 1:], jnp.zeros((2, 1), jnp.int32)], axis=1)
    next_live = jnp.concatenate([out_live[:, 1:], jnp.zeros((2, 1), jnp.int32)], axis=1)
    goes_on = valid & (within < jnp.sum(jnp.where(choice, next_live[:, None, :], 0), axis=2))
    onward = way_base + within + jnp.sum(jnp.where(choice, next_start[:, None, :], 0), axis=2)
    onward = jnp.clip(jnp.where(goes_on, onward, none_row), 0, none_row)

    source_of = jnp.arange(ep, dtype=jnp.int32)
    far = jnp.stack([(me - 1 - source_of) % ep, (source_of - me - 1) % ep])
    base = jnp.stack([lookup(in_start[way], far[way], steps) for way in (0, 1)])
    way_of = (codes >= tokens).astype(jnp.int32)
    spot_of = jnp.where(
        way_of == 1, rows + base[1][:, None] + codes - tokens, base[0][:, None] + codes
    )
    spot_of = jnp.where(codes >= 2 * tokens, 2 * rows + codes - 2 * tokens, spot_of)
    expert = jnp.clip(jnp.where(codes >= 0, spot_of, zero_row), 0, zero_row).reshape(-1)

    total = ep * capacity
    index = jnp.arange(total, dtype=jnp.int32) + 1
    here = (expert[:, None] // CHUNK == jnp.arange(2 * CHUNKS, dtype=jnp.int32)[None]).astype(
        jnp.bfloat16
    )
    inner = expert[:, None] % CHUNK == jnp.arange(CHUNK, dtype=jnp.int32)[None]
    parts = [
        jnp.where(inner, part[:, None], 0).astype(jnp.bfloat16)
        for part in (index // LANES, index % LANES)
    ]
    found = lax.dot_general(
        here,
        jnp.concatenate(parts, axis=1),
        (((0,), (0,)), ((), ())),
        preferred_element_type=jnp.float32,
    ).astype(jnp.int32)
    found = (found[:, :CHUNK] * LANES + found[:, CHUNK:]).reshape(2, rows)
    first_result = none_row + CHUNK
    result_pick = jnp.where(found > 0, first_result + found - 1, none_row)

    back = jnp.where(reach > 0, way_base + rank, none_row)
    mine = route_ids == me
    local = jnp.sum(jnp.where(mine, first_result + target - none_row, 0), axis=1) + none_row
    final = jnp.concatenate([jnp.clip(back, 0, none_row), local[None]], axis=0)
    return fits, pick, expert, result_pick, onward, final


def feed_forward(rows, gate_up, full_down):
    both = jnp.dot(rows, gate_up, preferred_element_type=jnp.float32)
    gate_pre, up_pre = jnp.split(both, 2, axis=1)
    hidden = (jax.nn.silu(gate_pre) * up_pre).astype(jnp.bfloat16)
    return jnp.dot(hidden, full_down, preferred_element_type=jnp.float32).astype(jnp.bfloat16)


def padded_exchange(normed, target, route_weights, weights, ep_size, capacity):
    row_count, features = normed.shape
    slots = jnp.arange(ep_size * capacity, dtype=jnp.int32)
    chosen = (slots[:, None] == target[None, :, 0]) | (slots[:, None] == target[None, :, 1])
    outbound = jnp.dot(
        chosen.astype(jnp.bfloat16), normed, preferred_element_type=jnp.float32
    ).astype(jnp.bfloat16)
    outbound = outbound.reshape(ep_size, capacity, features)
    arrived = lax.all_to_all(outbound, "ep", split_axis=0, concat_axis=0, tiled=True)
    result = lax.map(
        lambda rows: feed_forward(rows, *weights), arrived.reshape(-1, 128, features)
    )
    returned_rows = send_back(result.reshape(ep_size, capacity, features))
    returned_rows = returned_rows.reshape(ep_size * capacity, features)
    combined = jnp.zeros((row_count, features), jnp.float32)
    for column in range(target.shape[1]):
        picked = returned_rows[target[:, column]].astype(jnp.float32)
        combined = combined + route_weights[:, column : column + 1] * picked
    return combined.astype(jnp.bfloat16)


def per_device(
    tokens,
    norm_gain,
    route_ids,
    route_weights,
    w_gate,
    w_up,
    w_down,
    dispatch=dispatch,
    collect=collect,
    starts_of=stream_starts,
):
    row_count, features = tokens.shape
    ep_size = lax.axis_size("ep")
    capacity = row_count * GROUPS // ep_size
    floats = tokens.astype(jnp.float32)
    inverse = lax.rsqrt(jnp.mean(floats * floats, axis=1, keepdims=True) + epsilon)
    normed = (floats * inverse * norm_gain).astype(jnp.bfloat16)
    message, reach, rank, target, steps = plan_routes(route_ids, route_weights, capacity)
    arrived = lax.all_to_all(message, "ep", split_axis=0, concat_axis=0, tiled=True)
    fits, pick, expert, result_pick, onward, final = plan_streams(
        arrived, reach, rank, target, route_ids, steps, capacity, starts_of
    )
    expert_rows, *weights = dispatch(
        pick, expert, normed.reshape(row_count, -1, LANES), (w_gate[0], w_up[0], w_down[0])
    )
    result = feed_forward(expert_rows.reshape(-1, features), *weights)
    scale = arrived[:, capacity : 2 * capacity].reshape(-1, 1)
    result = (result.astype(jnp.float32) * scale).astype(jnp.bfloat16)
    result = result.reshape(-1, features // LANES, LANES)
    mixed = collect(result_pick, onward, final, result).reshape(row_count, features)
    return lax.cond(
        fits,
        lambda: mixed,
        lambda: padded_exchange(normed, target, route_weights, weights, ep_size, capacity),
    )


def solution(mesh):
    in_specs = (
        P(("grp", "ep", "tp"), None),
        P(),
        P(("grp", "ep", "tp"), None),
        P(("grp", "ep", "tp"), None),
        P("ep", None, "tp"),
        P("ep", None, "tp"),
        P("ep", "tp", None),
    )
    out_specs = P(("grp", "ep", "tp"), None)
    return jax.shard_map(
        per_device, mesh=mesh, in_specs=in_specs, out_specs=out_specs, check_vma=False
    )
```

```python
import functools

import jax
import jax.numpy as jnp
from jax import lax
from jax.experimental import pallas as pl
from jax.experimental.pallas import tpu as pltpu
from jax.sharding import PartitionSpec as P

GROUPS = 4

epsilon = 1e-06

CHUNK = 8
LAG = 6
CHUNKS = 238
BIAS = 6
SLOTS = 8
LANES = 128


def send_back(result):
    return lax.all_to_all(result, "ep", split_axis=0, concat_axis=0, tiled=True)


def ring_setup(others=()):
    ep = lax.axis_size("ep")
    me = lax.axis_index("ep")
    up, down = lax.rem(me + 1, ep), lax.rem(me + ep - 1, ep)
    peers = [{"ep": up}, {"ep": down}] + list(others)
    barrier = pltpu.get_barrier_semaphore()
    for peer in peers:
        pl.semaphore_signal(
            barrier, inc=1, device_id=peer, device_id_type=pl.DeviceIdType.MESH
        )
    pl.semaphore_wait(barrier, len(peers))
    return up, down


def chunk_copy(send, land, send_sem, recv_sem, peer, way, slot, chunk):
    return pltpu.make_async_remote_copy(
        src_ref=send.at[way, slot],
        dst_ref=land.at[way, chunk],
        send_sem=send_sem.at[way, slot],
        recv_sem=recv_sem.at[way, chunk],
        device_id={"ep": peer},
        device_id_type=pl.DeviceIdType.MESH,
    )


def ring_stream(peers, order, build, keep, send, land, send_sem, recv_sem):
    def receive(way, step):
        chunk = order(step)
        chunk_copy(send, land, send_sem, recv_sem, peers[way], way, 0, chunk).wait_recv()
        keep(way, chunk)

    def drain(step):
        slot = lax.rem(step, SLOTS)
        for way in (0, 1):
            chunk_copy(
                send, land, send_sem, recv_sem, peers[way], way, slot, order(step)
            ).wait_send()

    def body(step, carry):
        slot = lax.rem(step, SLOTS)

        @pl.when(step >= SLOTS)
        def _():
            drain(step - SLOTS)

        for way in (0, 1):

            @pl.when(step >= LAG)
            def _():
                receive(way, step - LAG)

            build(way, slot, order(step))
        for way in (0, 1):
            chunk_copy(
                send, land, send_sem, recv_sem, peers[way], way, slot, order(step)
            ).start()
        return carry

    lax.fori_loop(0, CHUNKS, body, 0)
    for step in range(CHUNKS - LAG, CHUNKS):
        for way in (0, 1):
            receive(way, step)
    for step in range(CHUNKS - SLOTS, CHUNKS):
        drain(step)


def half_copies(halves, wholes, half_sem, own_sem, half, other):
    remote, local = [], []
    for index, (part, whole, group) in enumerate(zip(halves, wholes, (0, 1, 0))):
        if part.shape[0] == whole.shape[0]:
            width = part.shape[1]
            at = (2 * group + half) * width
            place = whole.at[:, pl.ds(pl.multiple_of(at, width), width)]
        else:
            depth = part.shape[0]
            place = whole.at[pl.ds(pl.multiple_of(half * depth, depth), depth)]
        remote.append(
            pltpu.make_async_remote_copy(
                src_ref=part,
                dst_ref=place,
                send_sem=half_sem.at[0, index],
                recv_sem=half_sem.at[1, index],
                device_id=other,
                device_id_type=pl.DeviceIdType.MESH,
            )
        )
        local.append(pltpu.make_async_copy(part, place, own_sem.at[index]))
    return remote, local


def dispatch_kernel(
    pick_ref,
    expert_ref,
    own_ref,
    gate_half,
    up_half,
    down_half,
    out_ref,
    gate_up_whole,
    down_whole,
    store,
    send,
    land,
    send_sem,
    recv_sem,
    half_sem,
    own_sem,
    load_sem,
):
    rows = CHUNKS * CHUNK
    own_rows = own_ref.shape[0]
    load = pltpu.make_async_copy(own_ref, store.at[pl.ds(2 * rows, own_rows)], load_sem)
    load.start()
    half = lax.axis_index("tp")
    other = {"tp": 1 - half}
    peers = ring_setup([other])
    halves = (gate_half, up_half, down_half)
    wholes = (gate_up_whole, gate_up_whole, down_whole)
    remote, local = half_copies(halves, wholes, half_sem, own_sem, half, other)
    for copy in remote + local:
        copy.start()
    store[pl.ds(2 * rows + own_rows, 1)] = jnp.zeros((1,) + own_ref.shape[1:], own_ref.dtype)
    load.wait()

    def keep(way, chunk):
        store[pl.ds(way * rows + chunk * CHUNK, CHUNK)] = land[way, chunk]

    def build(way, slot, chunk):
        taken = [store[pick_ref[way, chunk * CHUNK + row]] for row in range(CHUNK)]
        for row, value in enumerate(taken):
            send[way, slot, row] = value

    ring_stream(peers, lambda step: step, build, keep, send, land, send_sem, recv_sem)

    batch = 2 * CHUNK

    def gather(block, carry):
        taken = [store[expert_ref[block * batch + row]] for row in range(batch)]
        for row, value in enumerate(taken):
            out_ref[block * batch + row] = value
        return carry

    lax.fori_loop(0, out_ref.shape[0] // batch, gather, 0)
    for copy in remote + local:
        copy.wait()


def collect_kernel(
    result_ref,
    onward_ref,
    final_ref,
    result,
    out_ref,
    store,
    send,
    land,
    send_sem,
    recv_sem,
    load_sem,
):
    rows = CHUNKS * CHUNK
    load = pltpu.make_async_copy(
        result, store.at[pl.ds(2 * rows + CHUNK, result.shape[0])], load_sem
    )
    load.start()
    up, down = ring_setup()
    store[pl.ds(2 * rows, 1)] = jnp.zeros((1,) + store.shape[1:], store.dtype)
    load.wait()

    def keep(way, chunk):
        store[pl.ds(way * rows + chunk * CHUNK, CHUNK)] = land[way, chunk]

    def build(way, slot, chunk):
        places = [chunk * CHUNK + row for row in range(CHUNK)]
        pairs = [(store[result_ref[way, at]], store[onward_ref[way, at]]) for at in places]
        for row, (here, beyond) in enumerate(pairs):
            total = here.astype(jnp.float32) + beyond.astype(jnp.float32)
            send[way, slot, row] = total.astype(send.dtype)

    ring_stream(
        (down, up),
        lambda step: CHUNKS - 1 - step,
        build,
        keep,
        send,
        land,
        send_sem,
        recv_sem,
    )

    def finish(block, carry):
        places = [block * CHUNK + row for row in range(CHUNK)]
        parts = [[store[final_ref[index, at]] for index in (2, 0, 1)] for at in places]
        for at, (local, above, below) in zip(places, parts):
            total = local.astype(jnp.float32) + above.astype(jnp.float32)
            total = total + below.astype(jnp.float32)
            out_ref[at] = total.astype(out_ref.dtype)
        return carry

    lax.fori_loop(0, out_ref.shape[0] // CHUNK, finish, 0)


def ring_scratch(store_rows, row_shape):
    return [
        pltpu.VMEM((store_rows,) + row_shape, jnp.bfloat16),
        pltpu.VMEM((2, SLOTS, CHUNK) + row_shape, jnp.bfloat16),
        pltpu.VMEM((2, CHUNKS, CHUNK) + row_shape, jnp.bfloat16),
        pltpu.SemaphoreType.DMA((2, SLOTS)),
        pltpu.SemaphoreType.DMA((2, CHUNKS)),
    ]


def ring_params(collective_id):
    return pltpu.CompilerParams(
        collective_id=collective_id, has_side_effects=True, vmem_limit_bytes=60 * 1024 * 1024
    )


SMEM = pl.BlockSpec(memory_space=pltpu.SMEM)
VMEM = pl.BlockSpec(memory_space=pltpu.VMEM)
ANY = pl.BlockSpec(memory_space=pl.ANY)


def dispatch(pick, expert, own, halves):
    row_shape = own.shape[1:]
    gate_half, _, down_half = halves
    wholes = [
        jax.ShapeDtypeStruct((gate_half.shape[0], 4 * gate_half.shape[1]), gate_half.dtype),
        jax.ShapeDtypeStruct((down_half.shape[0] * 2, down_half.shape[1]), down_half.dtype),
    ]
    return pl.pallas_call(
        dispatch_kernel,
        out_shape=[jax.ShapeDtypeStruct((expert.shape[0],) + row_shape, jnp.bfloat16)] + wholes,
        in_specs=[SMEM, SMEM, ANY, ANY, ANY, ANY],
        out_specs=[VMEM, ANY, ANY],
        scratch_shapes=ring_scratch(2 * CHUNKS * CHUNK + own.shape[0] + 1, row_shape)
        + [
            pltpu.SemaphoreType.DMA((2, 3)),
            pltpu.SemaphoreType.DMA((3,)),
            pltpu.SemaphoreType.DMA,
        ],
        compiler_params=ring_params(0),
        name="dispatch",
    )(pick, expert, own, *halves)


def collect(result_pick, onward, final, result):
    row_shape = result.shape[1:]
    return pl.pallas_call(
        collect_kernel,
        out_shape=jax.ShapeDtypeStruct((final.shape[1],) + row_shape, jnp.bfloat16),
        in_specs=[SMEM, SMEM, SMEM, ANY],
        out_specs=VMEM,
        scratch_shapes=ring_scratch(2 * CHUNKS * CHUNK + CHUNK + result.shape[0], row_shape)
        + [pltpu.SemaphoreType.DMA],
        compiler_params=ring_params(1),
        name="collect",
    )(result_pick, onward, final, result)


def starts_kernel(steps, counts_ref, starts_ref, lives_ref):
    shifts = (1, LANES - 1)
    start = [jnp.zeros((1, LANES), jnp.int32)] * 2
    live = [None, None]
    for distance in range(steps):
        for way in (0, 1):
            at = way * steps + distance
            if distance:
                start[way] = jnp.maximum(
                    start[way] + live[way],
                    pltpu.roll(start[way], shifts[way], axis=1) + LAG * CHUNK,
                )
            live[way] = counts_ref[at : at + 1]
            if distance:
                live[way] = pltpu.roll(live[way], shifts[way] * distance % LANES, axis=1)
            starts_ref[at : at + 1] = start[way]
            lives_ref[at : at + 1] = live[way]


def stream_starts(counts, steps):
    shape = jax.ShapeDtypeStruct(counts.shape, jnp.int32)
    return pl.pallas_call(
        functools.partial(starts_kernel, steps),
        out_shape=[shape, shape],
        in_specs=[VMEM],
        out_specs=[VMEM, VMEM],
        name="starts",
    )(counts)


def plan_routes(route_ids, route_weights, capacity):
    ep = lax.axis_size("ep")
    me = lax.axis_index("ep")
    tokens = route_ids.shape[0]
    steps = ep // 2 + ep // GROUPS
    low = jnp.min(route_ids, axis=1)
    high = jnp.max(route_ids, axis=1)
    ahead = jnp.maximum((low - me) % ep, (high - me) % ep)
    behind = jnp.maximum((me - low) % ep, (me - high) % ep)
    inside = (low <= me) & (me <= high)
    upward = ahead <= behind
    bias = jnp.arange(-BIAS, BIAS + 1, dtype=jnp.int32)[:, None]
    try_up = (ahead - behind)[None, :] <= bias
    ways = [
        jnp.where(inside, high - me, jnp.where(try_up, ahead, 0)),
        jnp.where(inside, me - low, jnp.where(try_up, 0, behind)),
    ]
    cost = jnp.maximum(jnp.sum(ways[0], axis=1), jnp.sum(ways[1], axis=1))[:, None]
    cost = (cost * 16 + jnp.abs(bias)) * 2 + (bias > 0).astype(jnp.int32)
    best = jnp.sum(jnp.where(cost == jnp.min(cost), bias, 0))
    upward = (ahead - behind) <= best
    reach = jnp.stack(
        [
            jnp.where(inside, high - me, jnp.where(upward, ahead, 0)),
            jnp.where(inside, me - low, jnp.where(upward, 0, behind)),
        ]
    )
    position = jnp.arange(tokens, dtype=jnp.int32)
    before = position[None, :] < position[:, None]
    further = (reach[:, None, :] > reach[:, :, None]) | (
        (reach[:, None, :] == reach[:, :, None]) & before[None]
    )
    rank = jnp.sum(further.astype(jnp.int32), axis=2)
    alive = jnp.sum(
        (reach[:, :, None] > jnp.arange(steps, dtype=jnp.int32)[None, None, :]).astype(jnp.int32),
        axis=1,
    )
    same = jnp.zeros((tokens, route_ids.shape[1]), jnp.int32)
    for column in range(route_ids.shape[1]):
        match = route_ids[:, :, None] == route_ids[None, None, :, column].reshape(1, 1, tokens)
        same = same + jnp.sum((match & before[:, None, :]).astype(jnp.int32), axis=2)
    target = route_ids * capacity + same
    goes_up = jnp.where(inside[:, None], route_ids > me, upward[:, None])
    code = jnp.where(goes_up, rank[0][:, None], tokens + rank[1][:, None])
    code = jnp.where(route_ids == me, 2 * tokens + position[:, None], code)
    slots = jnp.arange(ep * capacity, dtype=jnp.int32)
    sent_code = jnp.zeros((ep * capacity,), jnp.float32)
    sent_weight = jnp.zeros((ep * capacity,), jnp.float32)
    for column in range(route_ids.shape[1]):
        hit = slots[:, None] == target[None, :, column]
        sent_code = sent_code + jnp.sum(
            jnp.where(hit, (code[:, column] + 1).astype(jnp.float32)[None, :], 0.0), axis=1
        )
        sent_weight = sent_weight + jnp.sum(
            jnp.where(hit, route_weights[:, column][None, :], 0.0), axis=1
        )
    counts = alive.astype(jnp.float32).reshape(1, 2 * steps)
    message = jnp.concatenate(
        [
            sent_code.reshape(ep, capacity),
            sent_weight.reshape(ep, capacity),
            jnp.broadcast_to(counts, (ep, 2 * steps)),
        ],
        axis=1,
    )
    message = jnp.pad(message, ((0, 0), (0, LANES - message.shape[1])))
    return message, reach, rank, target, steps


def lookup(table, index, size):
    choice = index[..., None] == jnp.arange(size, dtype=jnp.int32)
    return jnp.sum(jnp.where(choice, table, 0), axis=-1)


def plan_streams(arrived, reach, rank, target, route_ids, steps, capacity, starts_of):
    ep = lax.axis_size("ep")
    me = lax.axis_index("ep")
    rows = CHUNKS * CHUNK
    tokens = rank.shape[1]
    codes = arrived[:, :capacity].astype(jnp.int32) - 1
    counts = arrived[:, 2 * capacity : 2 * capacity + 2 * steps].astype(jnp.int32)
    counts = jnp.tile(counts.T, (1, LANES // ep))
    starts, lives = starts_of(counts, steps)
    starts = starts.reshape(2, steps, LANES)
    lives = lives.reshape(2, steps, LANES)
    fits = jnp.max(jnp.where(lives > 0, starts + lives, 0)) <= rows

    column = jnp.arange(LANES, dtype=jnp.int32)

    def at_device(table, device):
        return jnp.sum(jnp.where(column[None, None, :] == device[:, None, None], table, 0), axis=2)

    spot = jnp.stack([me, me])
    previous = jnp.stack([(me + ep - 1) % ep, (me + 1) % ep])
    out_start, out_live = at_device(starts, spot), at_device(lives, spot)
    in_start, in_live = at_device(starts, previous), at_device(lives, previous)
    way_base = (jnp.arange(2, dtype=jnp.int32) * rows)[:, None]
    place = jnp.arange(rows, dtype=jnp.int32)

    def locate(start, live):
        distance = (
            jnp.sum((place[None, :, None] >= start[:, None, :]).astype(jnp.int32), axis=2) - 1
        )
        choice = distance[:, :, None] == jnp.arange(steps, dtype=jnp.int32)
        within = place[None] - jnp.sum(jnp.where(choice, start[:, None, :], 0), axis=2)
        valid = within < jnp.sum(jnp.where(choice, live[:, None, :], 0), axis=2)
        return choice, within, valid

    own_list = jnp.sum(
        jnp.where(
            rank[:, None, :] == jnp.arange(tokens, dtype=jnp.int32)[None, :, None],
            jnp.arange(tokens, dtype=jnp.int32)[None, None, :],
            0,
        ),
        axis=2,
    )
    own_list = jnp.pad(own_list, ((0, 0), (0, rows - tokens)))
    zero_row = 2 * rows + tokens
    choice, within, valid = locate(out_start, out_live)
    shifted = jnp.concatenate([jnp.zeros((2, 1), jnp.int32), in_start[:, :-1]], axis=1)
    source = way_base + within + jnp.sum(jnp.where(choice, shifted[:, None, :], 0), axis=2)
    source = jnp.where(choice[:, :, 0], 2 * rows + own_list, source)
    pick = jnp.clip(jnp.where(valid, source, zero_row), 0, zero_row)

    none_row = 2 * rows
    choice, within, valid = locate(in_start, in_live)
    next_start = jnp.concatenate([out_start[:, 1:], jnp.zeros((2, 1), jnp.int32)], axis=1)
    next_live = jnp.concatenate([out_live[:, 1:], jnp.zeros((2, 1), jnp.int32)], axis=1)
    goes_on = valid & (within < jnp.sum(jnp.where(choice, next_live[:, None, :], 0), axis=2))
    onward = way_base + within + jnp.sum(jnp.where(choice, next_start[:, None, :], 0), axis=2)
    onward = jnp.clip(jnp.where(goes_on, onward, none_row), 0, none_row)

    source_of = jnp.arange(ep, dtype=jnp.int32)
    far = jnp.stack([(me - 1 - source_of) % ep, (source_of - me - 1) % ep])
    base = jnp.stack([lookup(in_start[way], far[way], steps) for way in (0, 1)])
    way_of = (codes >= tokens).astype(jnp.int32)
    spot_of = jnp.where(
        way_of == 1, rows + base[1][:, None] + codes - tokens, base[0][:, None] + codes
    )
    spot_of = jnp.where(codes >= 2 * tokens, 2 * rows + codes - 2 * tokens, spot_of)
    expert = jnp.clip(jnp.where(codes >= 0, spot_of, zero_row), 0, zero_row).reshape(-1)

    total = ep * capacity
    index = jnp.arange(total, dtype=jnp.int32) + 1
    here = (expert[:, None] // CHUNK == jnp.arange(2 * CHUNKS, dtype=jnp.int32)[None]).astype(
        jnp.bfloat16
    )
    inner = expert[:, None] % CHUNK == jnp.arange(CHUNK, dtype=jnp.int32)[None]
    parts = [
        jnp.where(inner, part[:, None], 0).astype(jnp.bfloat16)
        for part in (index // LANES, index % LANES)
    ]
    found = lax.dot_general(
        here,
        jnp.concatenate(parts, axis=1),
        (((0,), (0,)), ((), ())),
        preferred_element_type=jnp.float32,
    ).astype(jnp.int32)
    found = (found[:, :CHUNK] * LANES + found[:, CHUNK:]).reshape(2, rows)
    first_result = none_row + CHUNK
    result_pick = jnp.where(found > 0, first_result + found - 1, none_row)

    back = jnp.where(reach > 0, way_base + rank, none_row)
    mine = route_ids == me
    local = jnp.sum(jnp.where(mine, first_result + target - none_row, 0), axis=1) + none_row
    final = jnp.concatenate([jnp.clip(back, 0, none_row), local[None]], axis=0)
    return fits, pick, expert, result_pick, onward, final


def feed_forward(rows, gate_up, full_down):
    both = jnp.dot(rows, gate_up, preferred_element_type=jnp.float32)
    gate_pre, up_pre = jnp.split(both, 2, axis=1)
    hidden = (jax.nn.silu(gate_pre) * up_pre).astype(jnp.bfloat16)
    return jnp.dot(hidden, full_down, preferred_element_type=jnp.float32).astype(jnp.bfloat16)


def padded_exchange(normed, target, route_weights, weights, ep_size, capacity):
    row_count, features = normed.shape
    slots = jnp.arange(ep_size * capacity, dtype=jnp.int32)
    chosen = (slots[:, None] == target[None, :, 0]) | (slots[:, None] == target[None, :, 1])
    outbound = jnp.dot(
        chosen.astype(jnp.bfloat16), normed, preferred_element_type=jnp.float32
    ).astype(jnp.bfloat16)
    outbound = outbound.reshape(ep_size, capacity, features)
    arrived = lax.all_to_all(outbound, "ep", split_axis=0, concat_axis=0, tiled=True)
    result = lax.map(
        lambda rows: feed_forward(rows, *weights), arrived.reshape(-1, 128, features)
    )
    returned_rows = send_back(result.reshape(ep_size, capacity, features))
    returned_rows = returned_rows.reshape(ep_size * capacity, features)
    combined = jnp.zeros((row_count, features), jnp.float32)
    for column in range(target.shape[1]):
        picked = returned_rows[target[:, column]].astype(jnp.float32)
        combined = combined + route_weights[:, column : column + 1] * picked
    return combined.astype(jnp.bfloat16)


def per_device(
    tokens,
    norm_gain,
    route_ids,
    route_weights,
    w_gate,
    w_up,
    w_down,
    dispatch=dispatch,
    collect=collect,
    starts_of=stream_starts,
):
    row_count, features = tokens.shape
    ep_size = lax.axis_size("ep")
    capacity = row_count * GROUPS // ep_size
    floats = tokens.astype(jnp.float32)
    inverse = lax.rsqrt(jnp.mean(floats * floats, axis=1, keepdims=True) + epsilon)
    normed = (floats * inverse * norm_gain).astype(jnp.bfloat16)
    message, reach, rank, target, steps = plan_routes(route_ids, route_weights, capacity)
    arrived = lax.all_to_all(message, "ep", split_axis=0, concat_axis=0, tiled=True)
    fits, pick, expert, result_pick, onward, final = plan_streams(
        arrived, reach, rank, target, route_ids, steps, capacity, starts_of
    )
    expert_rows, *weights = dispatch(
        pick, expert, normed.reshape(row_count, -1, LANES), (w_gate[0], w_up[0], w_down[0])
    )
    result = feed_forward(expert_rows.reshape(-1, features), *weights)
    scale = arrived[:, capacity : 2 * capacity].reshape(-1, 1)
    result = (result.astype(jnp.float32) * scale).astype(jnp.bfloat16)
    result = result.reshape(-1, features // LANES, LANES)
    mixed = collect(result_pick, onward, final, result).reshape(row_count, features)
    return lax.cond(
        fits,
        lambda: mixed,
        lambda: padded_exchange(normed, target, route_weights, weights, ep_size, capacity),
    )


def solution(mesh):
    in_specs = (
        P(("grp", "ep", "tp"), None),
        P(),
        P(("grp", "ep", "tp"), None),
        P(("grp", "ep", "tp"), None),
        P("ep", None, "tp"),
        P("ep", None, "tp"),
        P("ep", "tp", None),
    )
    out_specs = P(("grp", "ep", "tp"), None)
    return jax.shard_map(
        per_device, mesh=mesh, in_specs=in_specs, out_specs=out_specs, check_vma=False
    )
```
